512 devices in a mesh: ep: 32 (over z, x), tp: 16 (over y, core).
Axes of the slice: x: 4, y: 8, z: 8, core: 2. Of those that a mesh axis runs over, the one named last changes fastest.
Arguments:
- query_latent: bfloat16 [8192, 768], P('ep'), may hold values from -600 to 600
- shared_latent: bfloat16 [8192, 512], P('ep'), may hold values from -600 to 600
- rotary_key: bfloat16 [8192, 64], P('ep'), may hold values from -2500 to 2500
- query_gain: float32 [768], replicated, may hold values from 0.1 to 1.9
- shared_gain: float32 [512], replicated, may hold values from 0.1 to 1.9
- query_plain_weight: bfloat16 [768, 2048], P(None, 'tp'), may hold values from -0.21875 to 0.21875
- query_turn_weight: bfloat16 [768, 1024], P(None, 'tp'), may hold values from -0.21875 to 0.21875
- key_weight: bfloat16 [512, 2048], P(None, 'tp'), may hold values from -0.25 to 0.25
- value_weight: bfloat16 [512, 2048], P(None, 'tp'), may hold values from -0.25 to 0.25
- mixer_out_weight: bfloat16 [2048, 2048], P('tp'), may hold values from -1 to 1
- expert_input: bfloat16 [4096, 2048], P('ep'), may hold values from -600 to 600
- expert_gain: float32 [2048], replicated, may hold values from 0.1 to 1.9
- routing: int32 [4096, 4], P('ep'), may hold values from 0 to 31, all different within a row; in each aligned block of 128 rows (0 to 127, 128 to 255, ...) at most 21 rows name the same one
- routing_weight: float32 [4096, 4], P('ep'), may hold values from 0.05 to 1
- gate_weight: bfloat16 [32, 2048, 2048], P('ep', None, 'tp'), may hold values from -0.375 to 0.375
- up_weight: bfloat16 [32, 2048, 2048], P('ep', None, 'tp'), may hold values from -0.375 to 0.375
- down_weight: bfloat16 [32, 2048, 2048], P('ep', 'tp'), may hold values from -0.01953125 to 0.01953125
Outputs:
- mixer_output: bfloat16 [8192, 2048], P('ep')
- expert_output: bfloat16 [4096, 2048], P('ep')
The draws below stay inside these ranges and needn't reach their ends.
Inputs may be any that keep to these rules, and one draw needn't show every extreme that they name: `routing`: each row names 4 different experts. In each aligned block of 128 rows (the rows of one index of ep) no expert is named by more than 21 rows, and in some block some expert is named by exactly 21.
All inputs are finite; a program needn't handle non-finite values.
Results may differ from the reference program's by a relative error of at most 0.019.
Values may be sent and summed in bfloat16 or wider, within the bound.
A program may use at most 128 MiB of HBM per device.

```python
import math
import jax
import jax.numpy as jnp
import numpy as np
from jax import lax

D = 2048
HEADS = 16
NOPE = 128
ROPE = 64
VDIM = 128
Q_RANK = 768
KV_RANK = 512
FF = 2048
TOPK = 4
M_DEV = 128
SEQ = 8192
TOK_M = 4096
EXPERTS = 32
CAP_DEV = 21
N_EP = 32
N_TP = 16


def spread_normal(key, row_count, col_count):
    key_base = jax.random.fold_in(key, 0)
    base_draw = jnp.clip(jax.random.normal(key_base, (row_count, col_count), jnp.float32), -6.0, 6.0)
    return base_draw


def draw_query_latent(key, part):
    return spread_normal(jax.random.fold_in(key, 11), SEQ, Q_RANK).astype(jnp.bfloat16)


def draw_shared_latent(key, part):
    return spread_normal(jax.random.fold_in(key, 12), SEQ, KV_RANK).astype(jnp.bfloat16)


def draw_expert_input(key, part):
    return spread_normal(jax.random.fold_in(key, 13), TOK_M, D).astype(jnp.bfloat16)


def draw_rotary_key(key, part):
    key_base = jax.random.fold_in(jax.random.fold_in(key, 14), 0)
    base_draw = jnp.clip(jax.random.normal(key_base, (SEQ, ROPE), jnp.float32), -6.0, 6.0)
    return base_draw.astype(jnp.bfloat16)


def block_levels(key, extent, shards, least, top_value):
    level, own = 1.0, jax.random.fold_in(key, 6)
    for axis_at, parts in shards:
        steps = jnp.exp(jax.random.uniform(jax.random.fold_in(own, axis_at), (parts,), jnp.float32, least / len(shards), top_value / len(shards)))
        level = level * jnp.repeat(steps, extent[axis_at] // parts).reshape([-1 if axis == axis_at else 1 for axis in range(len(extent))])
    return level


def shared_out(stream_key, own, number, rows, count, top, reach, slope):
    order = jax.random.permutation(stream_key, count)
    crowded, ordinary = load_shares(count, rows * top, reach, slope, True), load_shares(count, rows * top, reach, slope, False)
    places = jnp.arange(count)

    def named(sizes, offset_by):
        used = int((sizes > 0).sum())
        fixed = max(1, used // 4)
        shifted = fixed + (places - fixed + offset_by * (used - fixed)) % max(1, count - fixed)
        return jnp.zeros((count,), jnp.int32).at[order[jnp.where(places < fixed, places, shifted)]].set(jnp.asarray(sizes, jnp.int32))

    sizes = jnp.where(number % 4 == 0, named(crowded, number // 4), named(ordinary, number - number // 4 - 1))
    mixed = jax.random.permutation(jax.random.fold_in(own, 3), count)
    source_of, receiver = mixed[0:count // 2 * 2:2], mixed[1:count // 2 * 2:2]
    margin = jnp.minimum(sizes[source_of] - 1, reach - sizes[receiver]) // 2
    margin = jnp.where((source_of == order[0]) | (receiver == order[0]) | (sizes[receiver] == 0), 0, jnp.maximum(margin, 0))
    shifted = jax.random.randint(jax.random.fold_in(own, 4), (count // 2,), 0, 1 << 20) % (margin + 1)
    sizes = sizes.at[source_of].add(-shifted).at[receiver].add(shifted)
    members = jnp.searchsorted(jnp.cumsum(sizes), jnp.arange(rows * top), side="right").astype(jnp.int32)
    listing = members.reshape(top, rows).T
    listing = listing[jax.random.permutation(jax.random.fold_in(own, 1), rows)]
    offset_by = jax.random.randint(jax.random.fold_in(own, 2), (rows, 1), 0, top)
    return jnp.take_along_axis(listing, (jnp.arange(top)[None, :] + offset_by) % top, axis=1)


def load_shares(number_of, total, most, skew, full):
    loads = [(1 << 20) // math.isqrt(rank ** skew) + 1 for rank in range(1, number_of + 1)]
    largest = most if full else min(most, max(-(-total // number_of), total * loads[0] // sum(loads)))
    least = 1 if total - largest >= number_of - 1 else 0
    counts, surplus = [largest] + [least] * (number_of - 1), total - largest - least * (number_of - 1)
    while surplus > 0:
        candidates = [i for i in range(1, number_of) if counts[i] < largest] or [i for i in range(1, number_of) if counts[i] < most]
        pool, left = sum([loads[i] for i in candidates]), surplus
        for i in candidates:
            addition = min(most - counts[i], max(1, left * loads[i] // pool), surplus)
            counts[i] = counts[i] + addition
            surplus = surplus - addition
    return np.array(counts)


def bell_draw(stream_key, extent, spread, reach, pieces=(), kind=jnp.bfloat16):
    values = spread * jax.random.normal(stream_key, extent, jnp.float32)
    if pieces:
        values = values * block_levels(stream_key, extent, pieces, -0.22, 0.18)
    return jnp.clip(values, -reach, reach).astype(kind)


def setup_inputs(seed: int = 0) -> dict:
    streams_of = jax.random.split(jax.random.key(seed), 18)
    query_latent = draw_query_latent(jax.random.fold_in(streams_of[17], 71), 0)
    shared_latent = draw_shared_latent(jax.random.fold_in(streams_of[17], 71), 0)
    rotary_key = draw_rotary_key(jax.random.fold_in(streams_of[17], 71), 0)
    query_gain = jnp.clip(1.0 + 0.18 * jax.random.normal(streams_of[3], (Q_RANK,), jnp.float32), 0.1, 1.9)
    shared_gain = jnp.clip(1.0 + 0.18 * jax.random.normal(streams_of[4], (KV_RANK,), jnp.float32), 0.1, 1.9)
    query_plain_weight = bell_draw(streams_of[5], (Q_RANK, HEADS * NOPE), Q_RANK ** -0.5, 0.21875, ((1, 16),))
    query_turn_weight = bell_draw(streams_of[6], (Q_RANK, HEADS * ROPE), Q_RANK ** -0.5, 0.21875, ((1, 16),))
    key_weight = bell_draw(streams_of[7], (KV_RANK, HEADS * NOPE), KV_RANK ** -0.5, 0.25, ((1, 16),))
    value_weight = bell_draw(streams_of[8], (KV_RANK, HEADS * VDIM), KV_RANK ** -0.5, 0.25, ((1, 16),))
    mixer_out_weight = bell_draw(streams_of[9], (HEADS * VDIM, D), (HEADS * VDIM // 64) ** -0.5, 1.0, ((0, 16),))
    expert_input = draw_expert_input(jax.random.fold_in(streams_of[17], 71), 0)
    expert_gain = jnp.clip(1.0 + 0.18 * jax.random.normal(streams_of[11], (D,), jnp.float32), 0.1, 1.9)
    routing_keys = jax.random.split(jax.random.fold_in(streams_of[12], 1), TOK_M // M_DEV)
    routing_turns = jax.random.permutation(jax.random.fold_in(streams_of[12], 3), TOK_M // M_DEV)
    routing = jax.vmap(lambda own, number: shared_out(jax.random.fold_in(streams_of[12], 2), own, number, M_DEV, EXPERTS, TOPK, CAP_DEV, 1))(routing_keys, routing_turns).reshape((TOK_M, TOPK))
    routing_weight = jnp.clip(jnp.exp(math.log(1.0) - 2.9957323 * jax.random.uniform(streams_of[13], (TOK_M, TOPK), jnp.float32) ** block_levels(streams_of[13], (TOK_M, TOPK), ((0, 32),), -0.2, 0.2)), 0.05, 1.0)
    gate_weight = bell_draw(streams_of[14], (EXPERTS, D, FF), (D // 9) ** -0.5, 0.375, ((0, 32), (2, 16)))
    up_weight = bell_draw(streams_of[15], (EXPERTS, D, FF), (D // 9) ** -0.5, 0.375, ((0, 32), (2, 16)))
    down_weight = bell_draw(streams_of[16], (EXPERTS, FF, D), (FF * 40) ** -0.5, 0.01953125, ((0, 32), (1, 16)))
    return dict(query_latent=query_latent, shared_latent=shared_latent, rotary_key=rotary_key, query_gain=query_gain, shared_gain=shared_gain, query_plain_weight=query_plain_weight, query_turn_weight=query_turn_weight, key_weight=key_weight, value_weight=value_weight, mixer_out_weight=mixer_out_weight, expert_input=expert_input, expert_gain=expert_gain, routing=routing, routing_weight=routing_weight, gate_weight=gate_weight, up_weight=up_weight, down_weight=down_weight)


EPSILON = 1e-06
CLAMP_LIMIT = 7.0
SLOPE = 1.702
ROTARY_BASE = 10000.0

def norm_rows(values, gains):
    widened = values.astype(jnp.float32)
    normed = widened * lax.rsqrt(lax.optimization_barrier(jnp.mean(widened * widened, axis=-1, keepdims=True)) + EPSILON)
    return (normed * gains).astype(jnp.bfloat16)

def rotary(values, position):
    half_dim = values.shape[-1] // 2
    frequency = ROTARY_BASE ** (-2.0 * jnp.arange(half_dim, dtype=jnp.float32) / values.shape[-1])
    angles = position.astype(jnp.float32)[:, None, None] * frequency[None, None, :]
    cosine = jnp.cos(angles)
    sine_part = jnp.sin(angles)
    lower = values[..., :half_dim]
    upper = values[..., half_dim:]
    return jnp.concatenate([lower * cosine - upper * sine_part, upper * cosine + lower * sine_part], axis=-1)

def mixer_reference(query_latent, shared_latent, rotary_key, query_gain, shared_gain, query_plain_weight, query_turn_weight, key_weight, value_weight, mixer_out_weight):
    seq_len = query_latent.shape[0]
    position = jnp.arange(seq_len, dtype=jnp.int32)
    query_normed = norm_rows(query_latent, query_gain)
    shared_normed = norm_rows(shared_latent, shared_gain)
    query_plain = jnp.dot(query_normed, query_plain_weight, preferred_element_type=jnp.float32).astype(jnp.bfloat16)
    query_plain = query_plain.reshape(seq_len, HEADS, NOPE)
    query_raw = jnp.dot(query_normed, query_turn_weight, preferred_element_type=jnp.float32)
    query_turned = rotary(query_raw.reshape(seq_len, HEADS, ROPE), position).astype(jnp.bfloat16)
    key_plain = jnp.dot(shared_normed, key_weight, preferred_element_type=jnp.float32).astype(jnp.bfloat16)
    key_plain = key_plain.reshape(seq_len, HEADS, NOPE).astype(jnp.float32)
    values = jnp.dot(shared_normed, value_weight, preferred_element_type=jnp.float32).astype(jnp.bfloat16)
    values = values.reshape(seq_len, HEADS, VDIM).astype(jnp.float32)
    key_turned = rotary(rotary_key.astype(jnp.float32).reshape(seq_len, 1, ROPE), position)
    key_turned = key_turned.astype(jnp.bfloat16).reshape(seq_len, ROPE).astype(jnp.float32)
    scaling = (NOPE + ROPE) ** (-0.5)
    block_rows = 256 if seq_len % 256 == 0 else seq_len
    block_count = seq_len // block_rows
    key_index = jnp.arange(seq_len, dtype=jnp.int32)

    def attend(first_row):
        plain_block = lax.dynamic_slice_in_dim(query_plain, first_row, block_rows, 0).astype(jnp.float32)
        turned_block = lax.dynamic_slice_in_dim(query_turned, first_row, block_rows, 0).astype(jnp.float32)
        scores = jnp.einsum('qhd,khd->hqk', plain_block, key_plain)
        scores = (scores + jnp.einsum('qhr,kr->hqk', turned_block, key_turned)) * scaling
        query_index = first_row + jnp.arange(block_rows, dtype=jnp.int32)
        visible = key_index[None, :] <= query_index[:, None]
        scores = jnp.where(visible[None], scores, -jnp.inf)
        peak = lax.optimization_barrier(jnp.max(scores, axis=-1, keepdims=True))
        probs = jnp.exp(scores - peak)
        totals = lax.optimization_barrier(jnp.sum(probs, axis=-1))
        rounded = lax.optimization_barrier(probs.astype(jnp.bfloat16))
        summed = jnp.einsum('hqk,khd->qhd', rounded.astype(jnp.float32), values)
        return (summed / jnp.transpose(totals)[:, :, None]).astype(jnp.bfloat16)
    starts = jnp.arange(block_count, dtype=jnp.int32) * block_rows
    heads_out = lax.map(attend, starts).reshape(seq_len, HEADS * VDIM)
    group_width = HEADS // N_TP * VDIM
    groups = jnp.transpose(heads_out.reshape(seq_len, N_TP, group_width), (1, 0, 2))
    weight_groups = mixer_out_weight.reshape(N_TP, group_width, D)

    def add_group(running, pair):
        part_rows, part_weight = pair
        term = jnp.dot(part_rows, part_weight, preferred_element_type=jnp.float32).astype(jnp.bfloat16)
        term = lax.optimization_barrier(term)
        return (running + term.astype(jnp.float32), None)
    summed, unused = lax.scan(add_group, jnp.zeros((seq_len, D), jnp.float32), (groups, weight_groups))
    return summed.astype(jnp.bfloat16)

def expert_reference(expert_input, expert_gain, routing, routing_weight, gate_weight, up_weight, down_weight):
    normed = norm_rows(expert_input, expert_gain)
    token_count = normed.shape[0]
    capacity_all = N_EP * CAP_DEV
    token_ids = jnp.arange(token_count, dtype=jnp.int32)
    ff_group = FF // N_TP

    def one_expert(running, inputs):
        expert, gate_part, up_part, down_part = inputs
        matches = routing == expert
        weight = lax.optimization_barrier(jnp.sum(jnp.where(matches, routing_weight, 0.0), axis=1))
        is_member = jnp.any(matches, axis=1)
        placed = jnp.cumsum(is_member.astype(jnp.int32)) - 1
        placed = jnp.where(is_member, placed, capacity_all).astype(jnp.int32)
        chosen = jnp.zeros((capacity_all,), jnp.int32).at[placed].set(token_ids, mode='drop')
        chosen_weight = jnp.zeros((capacity_all,), jnp.float32).at[placed].set(weight, mode='drop')
        picked = normed[chosen]
        gate_pre = jnp.minimum(jnp.dot(picked, gate_part, preferred_element_type=jnp.float32), CLAMP_LIMIT)
        up_pre = jnp.clip(jnp.dot(picked, up_part, preferred_element_type=jnp.float32), -CLAMP_LIMIT, CLAMP_LIMIT)
        hidden = ((up_pre + 1.0) * (gate_pre * jax.nn.sigmoid(SLOPE * gate_pre))).astype(jnp.bfloat16)
        grouped = hidden.reshape(capacity_all, N_TP, ff_group).astype(jnp.float32)
        down_groups = down_part.reshape(N_TP, ff_group, D).astype(jnp.float32)
        partial_value = jnp.einsum('mnf,nfd->nmd', grouped, down_groups).astype(jnp.bfloat16)
        partial_value = lax.optimization_barrier(partial_value)
        result = lax.optimization_barrier(jnp.sum(partial_value.astype(jnp.float32), axis=0)).astype(jnp.bfloat16)
        result = lax.optimization_barrier(result)
        running = running.at[chosen].add(chosen_weight[:, None] * result.astype(jnp.float32))
        return (running, None)
    experts = jnp.arange(gate_weight.shape[0], dtype=jnp.int32)
    total, unused = lax.scan(one_expert, jnp.zeros((token_count, D), jnp.float32), (experts, gate_weight, up_weight, down_weight))
    return total.astype(jnp.bfloat16)

def reference(query_latent, shared_latent, rotary_key, query_gain, shared_gain, query_plain_weight, query_turn_weight, key_weight, value_weight, mixer_out_weight, expert_input, expert_gain, routing, routing_weight, gate_weight, up_weight, down_weight):
    mixer_output = mixer_reference(query_latent, shared_latent, rotary_key, query_gain, shared_gain, query_plain_weight, query_turn_weight, key_weight, value_weight, mixer_out_weight)
    expert_output = expert_reference(expert_input, expert_gain, routing, routing_weight, gate_weight, up_weight, down_weight)
    return (mixer_output, expert_output)
```

```python
import functools
import math

import jax
import jax.numpy as jnp
from jax import lax
from jax.experimental import pallas as pl
from jax.experimental.pallas import tpu as pltpu
from jax.sharding import Mesh
from jax.sharding import PartitionSpec as P

MESH = pl.DeviceIdType.MESH
F32 = jnp.float32
BF16 = jnp.bfloat16
NOPE = 128
ROPE = 64
LANES = 128
EPSILON = 1e-06
CLAMP_LIMIT = 7.0
SLOPE = 1.702
ROTARY_BASE = 10000.0
NEGATIVE = -1e30
EP = ("z", "x")
TP = ("y", "c")
NX = 4


def dot(a, b, on_a=1, on_b=0):
    return lax.dot_general(a, b, (((on_a,), (on_b,)), ((), ())), preferred_element_type=F32)


def iota(shape, dim):
    return lax.broadcasted_iota(jnp.int32, shape, dim)


def normed(ref, gain_ref):
    wide = ref[...].astype(F32)
    wide = wide * lax.rsqrt(jnp.mean(wide * wide, axis=-1, keepdims=True) + EPSILON)
    return (wide * gain_ref[...]).astype(BF16)


def turned(u, cosine, sine):
    half = u.shape[0] // 2
    lower, upper = u[:half], u[half:]
    return jnp.concatenate([lower * cosine - upper * sine, upper * cosine + lower * sine], axis=0)


class Sender:
    def __init__(self):
        self.owed = []

    def copy(self, src, dst, send_sem, recv_sem, device):
        return pltpu.make_async_remote_copy(
            src_ref=src, dst_ref=dst, send_sem=send_sem, recv_sem=recv_sem,
            device_id=device, device_id_type=MESH,
        )

    def start(self, *what):
        made = self.copy(*what)
        made.start()
        self.owed.append(made.wait_send)

    def finish(self):
        for wait in self.owed:
            wait()


def ring_gather(send, axis, size, buf, slot, send_sem, recv_sem, pair=None):
    me = lax.axis_index(axis)
    ways = ({axis: lax.rem(me + 1, size)}, {axis: lax.rem(me + size - 1, size)})
    steps = size // 2
    rows = buf.shape[1] // 2

    def part(offset, half):
        return buf.at[slot(lax.rem(me + offset + size, size)), pl.ds(half * rows, rows)]

    def in_use(step, way, half):
        return step < steps or way == half

    def hop(step, way, half):
        ref = part((1 - step) if way == 0 else (step - 1), half)
        at = (way, step - 1, half)
        return (ref, ref, send_sem.at[at], recv_sem.at[at], ways[way])

    def hand(ref, at):
        if pair is not None:
            device, pair_send, pair_recv = pair
            send.start(ref, ref, pair_send.at[at], pair_recv.at[at], device)

    for half in range(2):
        for way in range(2):
            if in_use(1, way, half):
                send.start(*hop(1, way, half))
    if pair is not None:
        for half in range(2):
            hand(part(0, half), (0, steps, half))
    yield
    for step in range(1, steps + 1):
        for half in range(2):
            for way in range(2):
                if in_use(step, way, half):
                    at = (way, step - 1, half)
                    ref = part(-step if way == 0 else step, half)
                    send.copy(ref, ref, send_sem.at[at], recv_sem.at[at], ways[way]).wait_recv()
                    if step < steps and in_use(step + 1, way, half):
                        send.start(*hop(step + 1, way, half))
                    hand(ref, at)
        yield


def pair_arrived(send, size, axis, buf, slot, step, pair):
    device, pair_send, pair_recv = pair
    me = lax.axis_index(axis)
    steps = size // 2
    rows = buf.shape[1] // 2
    if step == 0:
        todo = [((0, steps, half), 0, half) for half in range(2)]
    else:
        todo = [
            ((way, step - 1, half), -step if way == 0 else step, half)
            for half in range(2) for way in range(2) if step < steps or way == half
        ]
    for at, offset, half in todo:
        ref = buf.at[slot(lax.rem(me + offset + size, size)), pl.ds(half * rows, rows)]
        send.copy(ref, ref, pair_send.at[at], pair_recv.at[at], device).wait_recv()


def product_scatter(send, size, product, part, given, ring, sems, pair_device, result):
    pair_send, pair_recv, send_sem, recv_sem = sems
    me, core = lax.axis_index("y"), lax.axis_index("c")
    ways = ({"y": lax.rem(me + 1, size)}, {"y": lax.rem(me + size - 1, size)})
    steps = size // 2
    rows = part.shape[2] // 2
    order = [steps]
    for k in range(steps - 1, 0, -1):
        order += [k, -k]
    order += [0]
    place = {offset % size: i for i, offset in enumerate(order)}
    seen = set()

    def at_piece(offset):
        return lax.rem(me + offset + size, size)

    def given_copy(offset):
        p, i = at_piece(offset), place[offset % size]
        return (part.at[1 - core, p], given.at[p], pair_send.at[i], pair_recv.at[i], pair_device)

    for offset in order:
        p = at_piece(offset)
        both = product(p).astype(BF16)
        part[0, p] = both[:, :LANES]
        part[1, p] = both[:, LANES:]
        send.start(*given_copy(offset))

    def in_use(step, way, half):
        return step >= 2 or way == half

    def arrival(step, way, half):
        at = (way, step - 1, half)
        ref = ring.at[way, step - 1, pl.ds(half * rows, rows)]
        send.copy(ref, ref, send_sem.at[at], recv_sem.at[at], ways[way]).wait_recv()
        return ring[way, step - 1, pl.ds(half * rows, rows)].astype(F32)

    def own(offset, half):
        if offset % size not in seen:
            seen.add(offset % size)
            send.copy(*given_copy(offset)).wait_recv()
        p, where = at_piece(offset), pl.ds(half * rows, rows)
        return part[core, p, where].astype(F32) + given[p, where].astype(F32)

    yield
    for step in range(1, steps + 1):
        for half in range(2):
            for way in range(2):
                if in_use(step, way, half):
                    offset = (steps - step + 1) * (1 if way == 0 else -1)
                    value = own(offset, half)
                    if step > 1 and in_use(step - 1, way, half):
                        value = value + arrival(step - 1, way, half)
                    p, where, at = at_piece(offset), pl.ds(half * rows, rows), (way, step - 1, half)
                    part[core, p, where] = value.astype(BF16)
                    send.start(
                        part.at[core, p, where], ring.at[way, step - 1, where],
                        send_sem.at[at], recv_sem.at[at], ways[way],
                    )
        yield
    for half in range(2):
        value = own(0, half)
        for way in range(2):
            if in_use(steps, way, half):
                value = value + arrival(steps, way, half)
        result[pl.ds(half * rows, rows)] = value.astype(BF16)


def exchange(send, nz, nx, src, dst, send_sem, recv_sem):
    count = nz * nx
    me = lax.axis_index("z") * nx + lax.axis_index("x")

    def out(d):
        to = lax.rem(me + d, count)
        return send.copy(
            src.at[to], dst.at[me], send_sem.at[d], recv_sem.at[d], {"z": to // nx, "x": lax.rem(to, nx)}
        )

    @pl.loop(1, count)
    def _(d):
        out(d).start()

    def wait():
        @pl.loop(1, count)
        def _(d):
            origin = lax.rem(me + count - d, count)
            send.copy(
                src.at[origin], dst.at[origin], send_sem.at[d], recv_sem.at[d],
                {"z": origin // nx, "x": lax.rem(origin, nx)},
            ).wait_recv()

    def sent():
        @pl.loop(1, count)
        def _(d):
            out(d).wait_send()

    send.owed.append(sent)
    dst[me] = src[me]
    return wait


def kernel(sizes, *refs):
    nz, nx, ny, cap, spaced = sizes
    (query_latent, shared_latent, rotary_key, cosine, sine, query_gain, shared_gain, plain_weight, turn_weight,
     key_weight, value_weight, mixer_weight, tokens, token_gain, routing, routing_weight, gate, up, down,
     mixer_out, expert_out, *scratch) = refs
    (out_rows, in_rows, pack, mix_high, mix_low, gath, gate_up, hidden, part_e, given_e, ring_e, back_out, back_in,
     result_e, queries, query_1, query_2, keys, peak, total, accum, share_out, stat_out, share_in, stat_in,
     heads, part_m, given_m, ring_m,
     s_a, r_a, s_g, r_g, sp_g, rp_g, sp_e, rp_e, s_e, r_e, s_b, r_b, s_f, r_f, sp_f, rp_f,
     s_q, r_q, s_k, r_k, s_o, r_o, s_t, r_t, sp_m, rp_m, s_m, r_m, s_h, r_h, sp_h, rp_h) = scratch
    z, x, y, core = (lax.axis_index(a) for a in ("z", "x", "y", "c"))
    count = nz * nx
    me = z * nx + x
    turn = 2 * y + core
    rows = query_latent.shape[0]
    other = {"c": 1 - core}
    send = Sender()

    barrier = pltpu.get_barrier_semaphore()

    @pl.loop(1, count)
    def _(d):
        to = lax.rem(me + d, count)
        pl.semaphore_signal(
            barrier, inc=1, device_id={"z": to // nx, "x": lax.rem(to, nx)}, device_id_type=MESH
        )

    for device in ({"y": lax.rem(y + 1, ny)}, {"y": lax.rem(y + ny - 1, ny)}, other):
        pl.semaphore_signal(barrier, inc=1, device_id=device, device_id_type=MESH)

    def expert_chain():
        width = pl.ds(pl.multiple_of(turn * LANES, LANES), LANES)
        wide = tokens[...].astype(F32)
        factor = lax.rsqrt(jnp.mean(wide * wide, axis=-1, keepdims=True) + EPSILON)
        own = (tokens[:, width].astype(F32) * factor * token_gain[:, width]).astype(BF16)
        count_of = own.shape[0]
        named = iota((count, count_of), 0)
        member = jnp.zeros((count, count_of), F32)
        weight = jnp.zeros((count, count_of), F32)
        for k in range(routing.shape[0]):
            hit = routing[k : k + 1, :] == named
            member = member + jnp.where(hit, 1.0, 0.0)
            weight = weight + jnp.where(hit, routing_weight[k : k + 1, :], 0.0)
        member = member.astype(BF16)
        earlier = jnp.where(
            iota((count_of, count_of), 0) < iota((count_of, count_of), 1), 1.0, 0.0
        ).astype(BF16)
        rank = dot(member, earlier).astype(BF16)
        slots = count * spaced
        shift = spaced.bit_length() - 1
        spread = jnp.where(
            lax.shift_right_logical(iota((slots, count), 0), shift) == iota((slots, count), 1), 1.0, 0.0
        ).astype(BF16)
        place = (iota((slots, count_of), 0) & (spaced - 1)).astype(F32)
        chosen = (dot(spread, member) > 0.5) & (dot(spread, rank) == place)
        high = weight.astype(BF16)
        low = (weight - high.astype(F32)).astype(BF16)
        mix_high[...] = jnp.where(chosen, dot(spread, high), 0.0).astype(BF16)
        mix_low[...] = jnp.where(chosen, dot(spread, low), 0.0).astype(BF16)
        out_rows[...] = dot(jnp.where(chosen, 1.0, 0.0).astype(BF16), own).astype(BF16).reshape(out_rows.shape)
        yield
        arrive = exchange(send, nz, nx, out_rows, in_rows, s_a, r_a)
        yield
        column = iota(pack.shape, 1)
        inner = column & (spaced - 1)
        goal = jnp.where(inner < cap, lax.shift_right_logical(column, shift) * cap + inner, -1)
        pack[...] = jnp.where(goal == iota(pack.shape, 0), 1.0, 0.0).astype(BF16)
        arrive()
        gath[turn] = dot(pack[...], in_rows[...].reshape(slots, LANES)).astype(BF16)
        slot = lambda p: 2 * p + core
        slot_other = lambda p: 2 * p + 1 - core
        pair = (other, sp_g, rp_g)
        ring = ring_gather(send, "y", ny, gath, slot, s_g, r_g, pair)
        steps = ny // 2
        next(ring)
        gate_up[...] = jnp.zeros_like(gate_up)

        def consume(piece):
            rows_of = pl.ds(pl.multiple_of(piece * LANES, LANES), LANES)
            both = jnp.concatenate([gate[rows_of, :], up[rows_of, :]], axis=1)
            gate_up[...] += dot(gath[piece], both)

        def consume_step(step, which):
            for offset in sorted({-step % ny, step % ny}):
                consume(which(lax.rem(y + offset, ny)))

        consume_step(0, slot)
        yield
        for step in range(1, steps + 1):
            next(ring)
            pair_arrived(send, ny, "y", gath, slot_other, step - 1, pair)
            consume_step(step - 1, slot_other)
            consume_step(step, slot)
            yield
        pair_arrived(send, ny, "y", gath, slot_other, steps, pair)
        consume_step(steps, slot_other)
        gate_pre = jnp.minimum(gate_up[:, :LANES], CLAMP_LIMIT)
        up_pre = jnp.clip(gate_up[:, LANES:], -CLAMP_LIMIT, CLAMP_LIMIT)
        hidden[...] = ((up_pre + 1.0) * (gate_pre * jax.nn.sigmoid(SLOPE * gate_pre))).astype(BF16)

        def product(p):
            return dot(hidden[...], down[:, pl.ds(pl.multiple_of(2 * LANES * p, 2 * LANES), 2 * LANES)])

        yield from product_scatter(
            send, ny, product, part_e, given_e, ring_e, (sp_e, rp_e, s_e, r_e), other, result_e
        )
        back_out[...] = dot(pack[...], result_e[...], 0, 0).astype(BF16).reshape(back_out.shape)
        arrive = exchange(send, nz, nx, back_out, back_in, s_b, r_b)
        yield
        arrive()
        back = back_in[...].reshape(slots, LANES)
        mixed = dot(mix_high[...], back, 0, 0) + dot(mix_low[...], back, 0, 0)
        expert_out[turn] = mixed.astype(BF16)
        pair = (other, sp_f, rp_f)
        yield from ring_gather(send, "y", ny, expert_out, slot, s_f, r_f, pair)
        for step in range(steps + 1):
            pair_arrived(send, ny, "y", expert_out, slot_other, step, pair)

    def mixer_chain():
        scale = (NOPE + ROPE) ** -0.5 * math.log2(math.e)
        latent = normed(query_latent, query_gain)
        queries[x, :rows] = dot(latent, plain_weight[...]).astype(BF16)
        raw = turned(dot(turn_weight[...], latent, 1, 1), cosine[...], sine[...])
        raw = jnp.concatenate([raw, jnp.zeros_like(raw)], axis=0)
        queries[x, rows:] = raw.T.astype(BF16)
        shared = normed(shared_latent, shared_gain)
        keys[z, :rows] = dot(shared, key_weight[...]).astype(BF16)
        keys[z, rows : 2 * rows] = dot(shared, value_weight[...]).astype(BF16)
        raw = turned(rotary_key[...].astype(F32), cosine[...], sine[...])
        raw = jnp.concatenate([raw[:, : rows // 2], raw[:, rows // 2 :]], axis=0)
        keys[z, 2 * rows :] = raw.T.astype(BF16)
        yield
        to_x = [lax.rem(x + d, nx) for d in range(nx)]
        from_x = [lax.rem(x + nx - d, nx) for d in range(nx)]
        for d in range(1, nx):
            send.start(queries.at[x], queries.at[x], s_q.at[d], r_q.at[d], {"x": to_x[d]})
        ring = ring_gather(send, "z", nz, keys, lambda p: p, s_k, r_k)
        next(ring)
        yield
        for d in range(1, nx):
            ref = queries.at[from_x[d]]
            send.copy(ref, ref, s_q.at[d], r_q.at[d], {"x": to_x[d]}).wait_recv()
        move = jnp.where(iota((LANES, LANES), 0) + ROPE == iota((LANES, LANES), 1), 1.0, 0.0).astype(BF16)
        for j in range(nx):
            span = pl.ds(j * rows, rows)
            plain, turned_part = queries[j, :rows], queries[j, rows:]
            query_1[span, :LANES] = plain
            query_1[span, LANES:] = turned_part
            query_2[span, :LANES] = plain
            query_2[span, LANES:] = dot(turned_part, move).astype(BF16)

        def attend(piece, own):
            half = rows // 2
            both = keys[piece, 2 * rows :]
            key_1 = jnp.concatenate([keys[piece, :half], both], axis=1)
            key_2 = jnp.concatenate([keys[piece, half:rows], both], axis=1)
            scores = jnp.concatenate(
                [dot(key_1, query_1[...], 1, 1), dot(key_2, query_2[...], 1, 1)], axis=0
            )
            if own:
                visible = iota(scores.shape, 0) + rows * x <= iota(scores.shape, 1)
                scores = jnp.where(visible, scores, NEGATIVE)
            highest = jnp.max(scores, axis=0, keepdims=True)
            if not own:
                highest = jnp.maximum(highest, peak[...])
            probs = jnp.exp2((scores - highest) * scale)
            summed = jnp.sum(probs, axis=0, keepdims=True)
            mixed = dot(keys[piece, rows : 2 * rows], probs.astype(BF16), 0, 0)
            if own:
                total[...] = summed
                accum[...] = mixed
            else:
                fade = jnp.exp2((peak[...] - highest) * scale)
                total[...] = total[...] * fade + summed
                accum[...] = accum[...] * fade + mixed
            peak[...] = highest

        attend(z, True)
        yield
        steps = nz // 2
        for step in range(1, steps + 1):
            next(ring)

            @pl.when(z >= step)
            def _():
                attend(lax.rem(z - step + nz, nz), False)

            if step < steps:
                @pl.when(z + step >= nz)
                def _():
                    attend(lax.rem(z + step, nz), False)

            yield
        share = (accum[...] / total[...]).astype(BF16)
        for j in range(nx):
            span = slice(j * rows, (j + 1) * rows)
            share_out[j] = share[:, span]
            stat = (8, rows)
            stat_out[j] = jnp.where(iota(stat, 0) == 0, peak[:, span], total[:, span])
        for d in range(1, nx):
            device = {"x": to_x[d]}
            send.start(share_out.at[to_x[d]], share_in.at[x], s_o.at[d], r_o.at[d], device)
            send.start(stat_out.at[to_x[d]], stat_in.at[x], s_t.at[d], r_t.at[d], device)
        share_in[x] = share_out[x]
        stat_in[x] = stat_out[x]
        yield
        for d in range(1, nx):
            device = {"x": to_x[d]}
            for ref, s, r in ((share_in, s_o, r_o), (stat_in, s_t, r_t)):
                ref = ref.at[from_x[d]]
                send.copy(ref, ref, s.at[d], r.at[d], device).wait_recv()
        peaks = [stat_in[j, 0:1, :] for j in range(nx)]
        highest = functools.reduce(jnp.maximum, peaks)
        factors = [stat_in[j, 1:2, :] * jnp.exp2((peaks[j] - highest) * scale) for j in range(nx)]
        merged = sum(share_in[j].astype(F32) * factors[j] for j in range(nx)) / sum(factors)
        heads[...] = merged.astype(BF16)

        def product(p):
            columns = pl.ds(pl.multiple_of(2 * LANES * p, 2 * LANES), 2 * LANES)
            return dot(heads[...], mixer_weight[:, columns], 0, 0)

        yield from product_scatter(
            send, ny, product, part_m, given_m, ring_m, (sp_m, rp_m, s_m, r_m), other, mixer_out.at[turn]
        )
        pair = (other, sp_h, rp_h)
        yield from ring_gather(send, "y", ny, mixer_out, lambda p: 2 * p + core, s_h, r_h, pair)
        for step in range(ny // 2 + 1):
            pair_arrived(send, ny, "y", mixer_out, lambda p: 2 * p + 1 - core, step, pair)

    chains = [expert_chain(), mixer_chain()]
    for chain in chains:
        next(chain)
    pl.semaphore_wait(barrier, count + 2)
    while chains:
        for chain in list(chains):
            try:
                next(chain)
            except StopIteration:
                chains.remove(chain)
    send.finish()


def per_device(sizes, query_latent, shared_latent, rotary_key, query_gain, shared_gain, plain_weight, turn_weight,
               key_weight, value_weight, mixer_weight, tokens, token_gain, routing, routing_weight, gate, up, down):
    nz, nx, ny, cap, spaced = sizes
    rows = query_latent.shape[0]
    position = (lax.axis_index(EP) * rows + jnp.arange(rows, dtype=jnp.int32)).astype(F32)
    half = ROPE // 2
    frequency = ROTARY_BASE ** (-2.0 * jnp.arange(half, dtype=F32) / ROPE)
    angles = position[None, :] * frequency[:, None]
    count, pieces = nz * nx, 2 * ny
    slots, packed = count * spaced, count * cap
    count_of = tokens.shape[0]
    vmem, dma = pltpu.VMEM, pltpu.SemaphoreType.DMA
    hops, handed = dma((2, ny // 2, 2)), dma((2, ny // 2 + 1, 2))
    scratch = [
        vmem((count, spaced, LANES), BF16), vmem((count, spaced, LANES), BF16), vmem((packed, slots), BF16),
        vmem((slots, count_of), BF16), vmem((slots, count_of), BF16), vmem((pieces, packed, LANES), BF16),
        vmem((packed, 2 * LANES), F32), vmem((packed, LANES), BF16), vmem((2, ny, packed, LANES), BF16),
        vmem((ny, packed, LANES), BF16), vmem((2, ny // 2, packed, LANES), BF16),
        vmem((count, spaced, LANES), BF16), vmem((count, spaced, LANES), BF16), vmem((packed, LANES), BF16),
        vmem((nx, 2 * rows, LANES), BF16), vmem((nx * rows, 2 * LANES), BF16), vmem((nx * rows, 2 * LANES), BF16),
        vmem((nz, 2 * rows + rows // 2, LANES), BF16), vmem((1, nx * rows), F32), vmem((1, nx * rows), F32),
        vmem((LANES, nx * rows), F32), vmem((nx, LANES, rows), BF16), vmem((nx, 8, rows), F32),
        vmem((nx, LANES, rows), BF16), vmem((nx, 8, rows), F32), vmem((LANES, rows), BF16),
        vmem((2, ny, rows, LANES), BF16), vmem((ny, rows, LANES), BF16), vmem((2, ny // 2, rows, LANES), BF16),
        dma((count,)), dma((count,)), hops, hops, handed, handed, dma((ny,)), dma((ny,)), hops, hops,
        dma((count,)), dma((count,)), hops, hops, handed, handed,
        dma((nx,)), dma((nx,)), dma((2, nz // 2, 2)), dma((2, nz // 2, 2)), dma((nx,)), dma((nx,)), dma((nx,)),
        dma((nx,)), dma((ny,)), dma((ny,)), hops, hops, hops, hops, handed, handed,
    ]
    spec = pl.BlockSpec(memory_space=pltpu.VMEM)
    operands = (
        query_latent, shared_latent, rotary_key.T, jnp.cos(angles), jnp.sin(angles), query_gain[None],
        shared_gain[None], plain_weight, turn_weight.T, key_weight, value_weight, mixer_weight, tokens,
        token_gain[None], routing.T, routing_weight.T, gate[0], up[0], down[0],
    )
    mixer_out, expert_out = pl.pallas_call(
        functools.partial(kernel, sizes),
        out_shape=(
            jax.ShapeDtypeStruct((pieces, rows, LANES), BF16),
            jax.ShapeDtypeStruct((pieces, count_of, LANES), BF16),
        ),
        in_specs=[spec] * len(operands),
        out_specs=(spec, spec),
        scratch_shapes=scratch,
        compiler_params=pltpu.CompilerParams(
            collective_id=0, has_side_effects=True, vmem_limit_bytes=56 * 1024 * 1024
        ),
        name="step",
    )(*operands)
    return tuple(a.transpose(1, 0, 2).reshape(a.shape[1], -1) for a in (mixer_out, expert_out))


def build(mesh, nx, cap, spaced):
    nz, ny = mesh.shape["ep"] // nx, mesh.shape["tp"] // 2
    finer = Mesh(mesh.devices.reshape(nz, nx, ny, 2), ("z", "x", "y", "c"))
    placed = (
        P(EP, None), P(EP, None), P(EP, None), P(), P(), P(None, TP), P(None, TP), P(None, TP), P(None, TP),
        P(TP, None), P(EP, None), P(), P(EP, None), P(EP, None), P(EP, None, TP), P(EP, None, TP), P(EP, TP, None),
    )
    return jax.shard_map(
        functools.partial(per_device, (nz, nx, ny, cap, spaced)),
        mesh=finer, in_specs=placed, out_specs=(P(EP, None), P(EP, None)), check_vma=False,
    )


def solution(mesh):
    return build(mesh, NX, 21, 32)
```

```python
import functools
import math

import jax
import jax.numpy as jnp
import numpy as np
from jax import lax
from jax.experimental import pallas as pl
from jax.experimental.pallas import tpu as pltpu
from jax.sharding import Mesh
from jax.sharding import PartitionSpec as P

MESH = pl.DeviceIdType.MESH
F32 = jnp.float32
BF16 = jnp.bfloat16
NOPE = 128
ROPE = 64
LANES = 128
EPSILON = 1e-06
CLAMP_LIMIT = 7.0
SLOPE = 1.702
ROTARY_BASE = 10000.0
NEGATIVE = -1e30
EP = ("z", "x")
TP = ("y", "c")
NX = 4
PARTS = 4


def dot(a, b, on_a=1, on_b=0):
    return lax.dot_general(a, b, (((on_a,), (on_b,)), ((), ())), preferred_element_type=F32)


def iota(shape, dim):
    return lax.broadcasted_iota(jnp.int32, shape, dim)


def normed(ref, gain_ref):
    wide = ref[...].astype(F32)
    wide = wide * lax.rsqrt(jnp.mean(wide * wide, axis=-1, keepdims=True) + EPSILON)
    return (wide * gain_ref[...]).astype(BF16)


def turned(u, cosine, sine):
    half = u.shape[0] // 2
    lower, upper = u[:half], u[half:]
    return jnp.concatenate([lower * cosine - upper * sine, upper * cosine + lower * sine], axis=0)


class Sender:
    def __init__(self):
        self.owed = []

    def copy(self, src, dst, send_sem, recv_sem, device):
        return pltpu.make_async_remote_copy(
            src_ref=src, dst_ref=dst, send_sem=send_sem, recv_sem=recv_sem,
            device_id=device, device_id_type=MESH,
        )

    def start(self, *what):
        made = self.copy(*what)
        made.start()
        self.owed.append(made.wait_send)

    def finish(self):
        for wait in self.owed:
            wait()


def cuts(rows, parts):
    edges = [rows * i // parts // 16 * 16 for i in range(parts)] + [rows]
    return [(lo, hi - lo) for lo, hi in zip(edges, edges[1:])]


def ring_gather(send, axis, size, piece, rows, parts, send_sem, recv_sem, pair=None):
    me = lax.axis_index(axis)
    ways = ({axis: lax.rem(me + 1, size)}, {axis: lax.rem(me + size - 1, size)})
    steps = size // 2

    def part(offset, i):
        return piece(lax.rem(me + offset + size, size), *cuts(rows, parts)[i])

    def in_use(step, way, i):
        return step < steps or way == 2 * i // parts

    def hop(step, way, i):
        ref = part((1 - step) if way == 0 else (step - 1), i)
        at = (way, step - 1, i)
        return (ref, ref, send_sem.at[at], recv_sem.at[at], ways[way])

    def hand(ref, at):
        if pair is not None:
            device, pair_send, pair_recv = pair
            send.start(ref, ref, pair_send.at[at], pair_recv.at[at], device)

    order = [(i + half * parts // 2, way) for i in range(parts // 2) for half in range(2) for way in range(2)]
    for i, way in order:
        if in_use(1, way, i):
            send.start(*hop(1, way, i))
    if pair is not None:
        for i in range(parts):
            hand(part(0, i), (0, steps, i))
    yield
    for step in range(1, steps + 1):
        for i, way in order:
            if in_use(step, way, i):
                at = (way, step - 1, i)
                ref = part(-step if way == 0 else step, i)
                send.copy(ref, ref, send_sem.at[at], recv_sem.at[at], ways[way]).wait_recv()
                if step < steps and in_use(step + 1, way, i):
                    send.start(*hop(step + 1, way, i))
                hand(ref, at)
        yield


def pair_arrived(send, size, axis, piece, rows, parts, step, pair):
    device, pair_send, pair_recv = pair
    me = lax.axis_index(axis)
    steps = size // 2
    if step == 0:
        todo = [((0, steps, i), 0, i) for i in range(parts)]
    else:
        todo = [
            ((way, step - 1, i), -step if way == 0 else step, i)
            for i in range(parts) for way in range(2) if step < steps or way == 2 * i // parts
        ]
    for at, offset, i in todo:
        ref = piece(lax.rem(me + offset + size, size), *cuts(rows, parts)[i])
        send.copy(ref, ref, pair_send.at[at], pair_recv.at[at], device).wait_recv()


def near_gather(send, piece, piece_other, rows, sems, device):
    send_sem, recv_sem, pair_send, pair_recv = sems
    size, half = 8, rows // 2
    me = lax.axis_index("y")

    def at_piece(offset):
        return lax.rem(me + offset + size, size)

    def span(k, way):
        return (way * half, half) if k == 3 else (0, rows)

    def copy(k, way, source, to):
        ref = piece(at_piece(source), *span(k, way))
        return (ref, ref, send_sem.at[way, k], recv_sem.at[way, k], {"y": at_piece(to)})

    def hand(which, at, offset, lo, count):
        ref = which(at_piece(offset), lo, count)
        return (ref, ref, pair_send.at[at], pair_recv.at[at], device)

    signs = (1, -1)
    for k, distance in ((1, 2), (0, 1)):
        for way, sign in enumerate(signs):
            send.start(*copy(k, way, 0, sign * distance))
    send.start(*hand(piece, (0, 4), 0, 0, rows))
    yield
    for k, distance in ((1, 2), (0, 1), (2, 3), (3, 4)):
        for way, sign in enumerate(signs):
            send.copy(*copy(k, way, -sign * distance, 0)).wait_recv()
            if k == 1:
                send.start(*copy(3, way, -sign * 2, sign * 2))
                send.start(*copy(2, way, -sign * 2, sign))
            send.start(*hand(piece, (way, k), -sign * distance, *span(k, way)))
        if k != 1:
            yield
    send.copy(*hand(piece_other, (0, 4), 0, 0, rows)).wait_recv()
    for k, distance in ((1, 2), (0, 1), (2, 3), (3, 4)):
        for way, sign in enumerate(signs):
            send.copy(*hand(piece_other, (way, k), -sign * distance, *span(k, way))).wait_recv()


class PairSum:
    def __init__(self, send, size, product, part, given, sems, device):
        self.send, self.size, self.product, self.part, self.given = send, size, product, part, given
        self.sems, self.device = sems, device
        self.me, self.core = lax.axis_index("y"), lax.axis_index("c")
        self.seen = set()

    def at(self, offset):
        return lax.rem(self.me + offset + self.size, self.size)

    def copy(self, offset):
        p, i = self.at(offset), offset % self.size
        pair_send, pair_recv = self.sems
        return (self.part.at[1 - self.core, p], self.given.at[p], pair_send.at[i], pair_recv.at[i], self.device)

    def make(self, *offsets):
        for offset in offsets:
            p = self.at(offset)
            both = self.product(p).astype(BF16)
            self.part[0, p] = both[:, :LANES]
            self.part[1, p] = both[:, LANES:]
            self.send.start(*self.copy(offset))

    def own(self, offset, where):
        if offset % self.size not in self.seen:
            self.seen.add(offset % self.size)
            self.send.copy(*self.copy(offset)).wait_recv()
        p = self.at(offset)
        return self.part[self.core, p, where].astype(F32) + self.given[p, where].astype(F32)

    def emit(self, offset, where, value, *to):
        self.part[self.core, self.at(offset), where] = value.astype(BF16)
        self.send.start(self.part.at[self.core, self.at(offset), where], *to)


def ring_scatter(send, size, sums, ring, parts, sems, result):
    send_sem, recv_sem = sems
    me = lax.axis_index("y")
    ways = ({"y": lax.rem(me + 1, size)}, {"y": lax.rem(me + size - 1, size)})
    steps = size // 2
    spans = [pl.ds(*cut) for cut in cuts(ring.shape[2], parts)]

    def in_use(step, way, i):
        return step >= 2 or way == 2 * i // parts

    def arrival(step, way, i):
        at = (way, step - 1, i)
        ref = ring.at[way, step - 1, spans[i]]
        send.copy(ref, ref, send_sem.at[at], recv_sem.at[at], ways[way]).wait_recv()
        return ring[way, step - 1, spans[i]].astype(F32)

    order = [(i + half * parts // 2, way) for i in range(parts // 2) for half in range(2) for way in range(2)]
    sums.make(steps)
    if steps > 1:
        sums.make(steps - 1, 1 - steps)
    for step in range(1, steps + 1):
        for i, way in order:
            if in_use(step, way, i):
                offset = (steps - step + 1) * (1 if way == 0 else -1)
                value = sums.own(offset, spans[i])
                if step > 1 and in_use(step - 1, way, i):
                    value = value + arrival(step - 1, way, i)
                at = (way, step - 1, i)
                sums.emit(
                    offset, spans[i], value, ring.at[way, step - 1, spans[i]],
                    send_sem.at[at], recv_sem.at[at], ways[way],
                )
        if steps - step > 1:
            sums.make(steps - step - 1, 1 + step - steps)
        elif steps - step == 1 or steps == 1:
            sums.make(0)
        yield
    for i in range(parts):
        value = sums.own(0, spans[i])
        for way in range(2):
            if in_use(steps, way, i):
                value = value + arrival(steps, way, i)
        result[spans[i]] = value.astype(BF16)


def near_scatter(send, sums, held, sems, result):
    send_sem, recv_sem = sems
    rows = held.shape[2]
    whole = pl.ds(0, rows)

    def span(k, way):
        return pl.ds(way * (rows // 2), rows // 2) if k == 1 else whole

    def to(k, way, distance):
        sign = 1 - 2 * way
        return (
            held.at[way, k, span(k, way)], send_sem.at[way, k], recv_sem.at[way, k],
            {"y": sums.at(sign * distance)},
        )

    def arrival(k, way):
        ref = held.at[way, k, span(k, way)]
        send.copy(ref, *to(k, way, 1)).wait_recv()
        return held[way, k, span(k, way)].astype(F32)

    sums.make(4, 3, -3, 2, -2)
    for way, sign in enumerate((1, -1)):
        sums.emit(4 * sign, span(1, way), sums.own(4 * sign, span(1, way)), *to(1, way, 2))
    for way, sign in enumerate((1, -1)):
        sums.emit(3 * sign, whole, sums.own(3 * sign, whole), *to(0, way, 1))
    sums.make(1, -1, 0)
    yield
    for way, sign in enumerate((1, -1)):
        value = sums.own(2 * sign, whole) + arrival(0, way)
        far = arrival(1, way)
        pad = jnp.zeros_like(far)
        value = value + jnp.concatenate([far, pad] if way == 0 else [pad, far], axis=0)
        sums.emit(2 * sign, whole, value, *to(3, way, 2))
    for way, sign in enumerate((1, -1)):
        sums.emit(sign, whole, sums.own(sign, whole), *to(2, way, 1))
    yield
    value = sums.own(0, whole)
    for k in (2, 3):
        for way in range(2):
            value = value + arrival(k, way)
    result[...] = value.astype(BF16)


def exchange(send, nz, nx, src, dst, send_sem, recv_sem):
    count = nz * nx
    me = lax.axis_index("z") * nx + lax.axis_index("x")

    def out(d):
        to = lax.rem(me + d, count)
        return send.copy(
            src.at[to], dst.at[me], send_sem.at[d], recv_sem.at[d], {"z": to // nx, "x": lax.rem(to, nx)}
        )

    @pl.loop(1, count)
    def _(d):
        out(d).start()

    def wait():
        @pl.loop(1, count)
        def _(d):
            origin = lax.rem(me + count - d, count)
            send.copy(
                src.at[origin], dst.at[origin], send_sem.at[d], recv_sem.at[d],
                {"z": origin // nx, "x": lax.rem(origin, nx)},
            ).wait_recv()

    def sent():
        @pl.loop(1, count)
        def _(d):
            out(d).wait_send()

    send.owed.append(sent)
    dst[me] = src[me]
    return wait


def kernel(sizes, *refs):
    nz, nx, ny, cap, spaced = sizes
    (query_latent, shared_latent, rotary_key, inside_cos, inside_sin, block_cos, block_sin, query_gain, shared_gain, plain_weight, turn_weight,
     key_weight, value_weight, mixer_weight, tokens, token_gain, routing, routing_weight, gate, up, down,
     mixer_out, expert_out, *scratch) = refs
    (out_rows, in_rows, pack, mix_high, mix_low, gath, gate_up, hidden, part_e, given_e, ring_e, back_out, back_in,
     result_e, queries, query_1, query_2, keys, peak, total, accum, share_out, stat_out, share_in, stat_in,
     heads, part_m, given_m, ring_m,
     s_a, r_a, s_g, r_g, sp_g, rp_g, sp_e, rp_e, s_e, r_e, s_b, r_b, s_f, r_f, sp_f, rp_f,
     s_q, r_q, s_k, r_k, s_o, r_o, s_t, r_t, sp_m, rp_m, s_m, r_m, s_h, r_h, sp_h, rp_h) = scratch
    z, x, y, core = (lax.axis_index(a) for a in ("z", "x", "y", "c"))
    count = nz * nx
    me = z * nx + x
    turn = 2 * y + core
    rows = query_latent.shape[0]
    other = {"c": 1 - core}
    send = Sender()

    barrier = pltpu.get_barrier_semaphore()

    @pl.loop(1, count)
    def _(d):
        to = lax.rem(me + d, count)
        pl.semaphore_signal(
            barrier, inc=1, device_id={"z": to // nx, "x": lax.rem(to, nx)}, device_id_type=MESH
        )

    greeted = [{"y": lax.rem(y + d + ny, ny)} for d in ((1, -1, 2, -2) if ny == 8 else (1, -1))] + [other]
    for device in greeted:
        pl.semaphore_signal(barrier, inc=1, device_id=device, device_id_type=MESH)

    def gather_columns(ref, sems):
        def piece(p, lo, size):
            return ref.at[pl.ds(lo, size), pl.ds(pl.multiple_of((2 * p + core) * LANES, LANES), LANES)]

        def piece_other(p, lo, size):
            return ref.at[pl.ds(lo, size), pl.ds(pl.multiple_of((2 * p + 1 - core) * LANES, LANES), LANES)]

        if ny == 8:
            yield from near_gather(send, piece, piece_other, ref.shape[0], sems, other)
        else:
            pair = (other, *sems[2:])
            yield from ring_gather(send, "y", ny, piece, ref.shape[0], 2, *sems[:2], pair)
            for step in range(ny // 2 + 1):
                pair_arrived(send, ny, "y", piece_other, ref.shape[0], 2, step, pair)

    def expert_chain():
        width = pl.ds(pl.multiple_of(turn * LANES, LANES), LANES)
        wide = tokens[...].astype(F32)
        factor = lax.rsqrt(jnp.mean(wide * wide, axis=-1, keepdims=True) + EPSILON)
        own = (tokens[:, width].astype(F32) * factor * token_gain[:, width]).astype(BF16)
        count_of = own.shape[0]
        named = iota((count, count_of), 0)
        member = jnp.zeros((count, count_of), F32)
        weight = jnp.zeros((count, count_of), F32)
        for k in range(routing.shape[0]):
            hit = routing[k : k + 1, :] == named
            member = member + jnp.where(hit, 1.0, 0.0)
            weight = weight + jnp.where(hit, routing_weight[k : k + 1, :], 0.0)
        member = member.astype(BF16)
        earlier = jnp.where(
            iota((count_of, count_of), 0) < iota((count_of, count_of), 1), 1.0, 0.0
        ).astype(BF16)
        rank = dot(member, earlier).astype(BF16)
        slots = count * spaced

        def block(line):
            return ((line.astype(F32) + 0.5) * (1.0 / spaced)).astype(jnp.int32)

        spread = jnp.where(block(iota((slots, count), 0)) == iota((slots, count), 1), 1.0, 0.0).astype(BF16)
        line = iota((slots, count_of), 0)
        place = (line - block(line) * spaced).astype(F32)
        chosen = (dot(spread, member) > 0.5) & (dot(spread, rank) == place)
        high = weight.astype(BF16)
        low = (weight - high.astype(F32)).astype(BF16)
        mix_high[...] = jnp.where(chosen, dot(spread, high), 0.0).astype(BF16)
        mix_low[...] = jnp.where(chosen, dot(spread, low), 0.0).astype(BF16)
        out_rows[...] = dot(jnp.where(chosen, 1.0, 0.0).astype(BF16), own).astype(BF16).reshape(out_rows.shape)
        yield
        arrive = exchange(send, nz, nx, out_rows, in_rows, s_a, r_a)
        yield
        column = iota(pack.shape, 1)
        inner = column - block(column) * spaced
        goal = jnp.where(inner < cap, block(column) * cap + inner, -1)
        pack[...] = jnp.where(goal == iota(pack.shape, 0), 1.0, 0.0).astype(BF16)
        arrive()
        gath[turn] = dot(pack[...], in_rows[...].reshape(slots, LANES)).astype(BF16)
        slot = lambda p: 2 * p + core
        slot_other = lambda p: 2 * p + 1 - core
        packed = gath.shape[1]
        piece = lambda p, lo, size: gath.at[slot(p), pl.ds(lo, size)]
        piece_other = lambda p, lo, size: gath.at[slot_other(p), pl.ds(lo, size)]
        pair = (other, sp_g, rp_g)
        ring = ring_gather(send, "y", ny, piece, packed, PARTS, s_g, r_g, pair)
        steps = ny // 2
        next(ring)
        gate_up[...] = jnp.zeros_like(gate_up)

        def consume(piece):
            rows_of = pl.ds(pl.multiple_of(piece * LANES, LANES), LANES)
            both = jnp.concatenate([gate[rows_of, :], up[rows_of, :]], axis=1)
            gate_up[...] += dot(gath[piece], both)

        def consume_step(step, which):
            for offset in sorted({-step % ny, step % ny}):
                consume(which(lax.rem(y + offset, ny)))

        consume_step(0, slot)
        yield
        for step in range(1, steps + 1):
            next(ring)
            pair_arrived(send, ny, "y", piece_other, packed, PARTS, step - 1, pair)
            consume_step(step - 1, slot_other)
            consume_step(step, slot)
            yield
        pair_arrived(send, ny, "y", piece_other, packed, PARTS, steps, pair)
        consume_step(steps, slot_other)
        gate_pre = jnp.minimum(gate_up[:, :LANES], CLAMP_LIMIT)
        up_pre = jnp.clip(gate_up[:, LANES:], -CLAMP_LIMIT, CLAMP_LIMIT)
        hidden[...] = ((up_pre + 1.0) * (gate_pre * jax.nn.sigmoid(SLOPE * gate_pre))).astype(BF16)

        def product(p):
            return dot(hidden[...], down[:, pl.ds(pl.multiple_of(2 * LANES * p, 2 * LANES), 2 * LANES)])

        sums = PairSum(send, ny, product, part_e, given_e, (sp_e, rp_e), other)
        yield from ring_scatter(send, ny, sums, ring_e, PARTS, (s_e, r_e), result_e)
        back_out[...] = dot(pack[...], result_e[...], 0, 0).astype(BF16).reshape(back_out.shape)
        arrive = exchange(send, nz, nx, back_out, back_in, s_b, r_b)
        yield
        arrive()
        back = back_in[...].reshape(slots, LANES)
        mixed = dot(mix_high[...], back, 0, 0) + dot(mix_low[...], back, 0, 0)
        expert_out[:, width] = mixed.astype(BF16)
        yield from gather_columns(expert_out, (s_f, r_f, sp_f, rp_f))

    def mixer_chain():
        scale = (NOPE + ROPE) ** -0.5 * math.log2(math.e)
        mine = iota(block_cos.shape, 1) == me
        cos_b = jnp.sum(jnp.where(mine, block_cos[...], 0.0), axis=1, keepdims=True)
        sin_b = jnp.sum(jnp.where(mine, block_sin[...], 0.0), axis=1, keepdims=True)
        cosine = inside_cos[...] * cos_b - inside_sin[...] * sin_b
        sine = inside_sin[...] * cos_b + inside_cos[...] * sin_b
        latent = normed(query_latent, query_gain)
        queries[x, :rows] = dot(latent, plain_weight[...]).astype(BF16)
        raw = turned(dot(turn_weight[...], latent, 1, 1), cosine, sine)
        raw = jnp.concatenate([raw, jnp.zeros_like(raw)], axis=0)
        queries[x, rows:] = raw.T.astype(BF16)
        shared = normed(shared_latent, shared_gain)
        keys[z, :rows] = dot(shared, key_weight[...]).astype(BF16)
        keys[z, rows : 2 * rows] = dot(shared, value_weight[...]).astype(BF16)
        raw = turned(rotary_key[...].astype(F32), cosine, sine)
        raw = jnp.concatenate([raw[:, : rows // 2], raw[:, rows // 2 :]], axis=0)
        keys[z, 2 * rows :] = raw.T.astype(BF16)
        yield
        to_x = [lax.rem(x + d, nx) for d in range(nx)]
        from_x = [lax.rem(x + nx - d, nx) for d in range(nx)]
        for d in range(1, nx):
            send.start(queries.at[x], queries.at[x], s_q.at[d], r_q.at[d], {"x": to_x[d]})
        ring = ring_gather(
            send, "z", nz, lambda p, lo, size: keys.at[p, pl.ds(lo, size)], keys.shape[1], 2, s_k, r_k
        )
        next(ring)
        yield
        for d in range(1, nx):
            ref = queries.at[from_x[d]]
            send.copy(ref, ref, s_q.at[d], r_q.at[d], {"x": to_x[d]}).wait_recv()
        move = jnp.where(iota((LANES, LANES), 0) + ROPE == iota((LANES, LANES), 1), 1.0, 0.0).astype(BF16)
        for j in range(nx):
            span = pl.ds(j * rows, rows)
            plain, turned_part = queries[j, :rows], queries[j, rows:]
            query_1[span, :LANES] = plain
            query_1[span, LANES:] = turned_part
            query_2[span, :LANES] = plain
            query_2[span, LANES:] = dot(turned_part, move).astype(BF16)

        def attend(piece, own):
            half = rows // 2
            both = keys[piece, 2 * rows :]
            key_1 = jnp.concatenate([keys[piece, :half], both], axis=1)
            key_2 = jnp.concatenate([keys[piece, half:rows], both], axis=1)
            scores = jnp.concatenate(
                [dot(key_1, query_1[...], 1, 1), dot(key_2, query_2[...], 1, 1)], axis=0
            )
            if own:
                visible = iota(scores.shape, 0) + rows * x <= iota(scores.shape, 1)
                scores = jnp.where(visible, scores, NEGATIVE)
            highest = jnp.max(scores, axis=0, keepdims=True)
            if not own:
                highest = jnp.maximum(highest, peak[...])
            probs = jnp.exp2((scores - highest) * scale)
            summed = jnp.sum(probs, axis=0, keepdims=True)
            mixed = dot(keys[piece, rows : 2 * rows], probs.astype(BF16), 0, 0)
            if own:
                total[...] = summed
                accum[...] = mixed
            else:
                fade = jnp.exp2((peak[...] - highest) * scale)
                total[...] = total[...] * fade + summed
                accum[...] = accum[...] * fade + mixed
            peak[...] = highest

        attend(z, True)
        yield
        steps = nz // 2
        for step in range(1, steps + 1):
            next(ring)

            @pl.when(z >= step)
            def _():
                attend(lax.rem(z - step + nz, nz), False)

            if step < steps:
                @pl.when(z + step >= nz)
                def _():
                    attend(lax.rem(z + step, nz), False)

            yield
        share = (accum[...] / total[...]).astype(BF16)
        for j in range(nx):
            span = slice(j * rows, (j + 1) * rows)
            share_out[j] = share[:, span]
            stat = (8, rows)
            stat_out[j] = jnp.where(iota(stat, 0) == 0, peak[:, span], total[:, span])
        for d in range(1, nx):
            device = {"x": to_x[d]}
            send.start(share_out.at[to_x[d]], share_in.at[x], s_o.at[d], r_o.at[d], device)
            send.start(stat_out.at[to_x[d]], stat_in.at[x], s_t.at[d], r_t.at[d], device)
        share_in[x] = share_out[x]
        stat_in[x] = stat_out[x]
        yield
        for d in range(1, nx):
            device = {"x": to_x[d]}
            for ref, s, r in ((share_in, s_o, r_o), (stat_in, s_t, r_t)):
                ref = ref.at[from_x[d]]
                send.copy(ref, ref, s.at[d], r.at[d], device).wait_recv()
        peaks = [stat_in[j, 0:1, :] for j in range(nx)]
        highest = functools.reduce(jnp.maximum, peaks)
        factors = [stat_in[j, 1:2, :] * jnp.exp2((peaks[j] - highest) * scale) for j in range(nx)]
        merged = sum(share_in[j].astype(F32) * factors[j] for j in range(nx)) / sum(factors)
        heads[...] = merged.astype(BF16)

        def product(p):
            columns = pl.ds(pl.multiple_of(2 * LANES * p, 2 * LANES), 2 * LANES)
            return dot(heads[...], mixer_weight[:, columns], 0, 0)

        sums = PairSum(send, ny, product, part_m, given_m, (sp_m, rp_m), other)
        result = mixer_out.at[:, pl.ds(pl.multiple_of(turn * LANES, LANES), LANES)]
        if ny == 8:
            yield from near_scatter(send, sums, ring_m, (s_m, r_m), result)
        else:
            yield from ring_scatter(send, ny, sums, ring_m, 2, (s_m, r_m), result)
        yield from gather_columns(mixer_out, (s_h, r_h, sp_h, rp_h))

    chains = [expert_chain(), mixer_chain()]
    for chain in chains:
        next(chain)
    pl.semaphore_wait(barrier, count - 1 + len(greeted))
    while chains:
        for chain in list(chains):
            try:
                next(chain)
            except StopIteration:
                chains.remove(chain)
    send.finish()


def per_device(sizes, query_latent, shared_latent, rotary_key, query_gain, shared_gain, plain_weight, turn_weight,
               key_weight, value_weight, mixer_weight, tokens, token_gain, routing, routing_weight, gate, up, down):
    nz, nx, ny, cap, spaced = sizes
    rows = query_latent.shape[0]
    count, pieces = nz * nx, 2 * ny
    frequency = ROTARY_BASE ** (-2.0 * np.arange(ROPE // 2) / ROPE)
    inside = frequency[:, None] * np.arange(rows)
    blocks = frequency[:, None] * (np.arange(count) * rows)
    tables = [jnp.asarray(f(a), F32) for a in (inside, blocks) for f in (np.cos, np.sin)]
    slots, packed = count * spaced, count * cap
    count_of = tokens.shape[0]
    vmem, dma = pltpu.VMEM, pltpu.SemaphoreType.DMA
    hops, handed = dma((2, ny // 2, PARTS)), dma((2, ny // 2 + 1, PARTS))
    if ny == 8:
        hops_m, hops_h, handed_h = dma((2, 4)), dma((2, 4)), dma((2, 5))
    else:
        hops_m, hops_h, handed_h = hops, hops, handed
    scratch = [
        vmem((count, spaced, LANES), BF16), vmem((count, spaced, LANES), BF16), vmem((packed, slots), BF16),
        vmem((slots, count_of), BF16), vmem((slots, count_of), BF16), vmem((pieces, packed, LANES), BF16),
        vmem((packed, 2 * LANES), F32), vmem((packed, LANES), BF16), vmem((2, ny, packed, LANES), BF16),
        vmem((ny, packed, LANES), BF16), vmem((2, ny // 2, packed, LANES), BF16),
        vmem((count, spaced, LANES), BF16), vmem((count, spaced, LANES), BF16), vmem((packed, LANES), BF16),
        vmem((nx, 2 * rows, LANES), BF16), vmem((nx * rows, 2 * LANES), BF16), vmem((nx * rows, 2 * LANES), BF16),
        vmem((nz, 2 * rows + rows // 2, LANES), BF16), vmem((1, nx * rows), F32), vmem((1, nx * rows), F32),
        vmem((LANES, nx * rows), F32), vmem((nx, LANES, rows), BF16), vmem((nx, 8, rows), F32),
        vmem((nx, LANES, rows), BF16), vmem((nx, 8, rows), F32), vmem((LANES, rows), BF16),
        vmem((2, ny, rows, LANES), BF16), vmem((ny, rows, LANES), BF16), vmem((2, ny // 2, rows, LANES), BF16),
        dma((count,)), dma((count,)), hops, hops, handed, handed, dma((ny,)), dma((ny,)), hops, hops,
        dma((count,)), dma((count,)), hops_h, hops_h, handed_h, handed_h,
        dma((nx,)), dma((nx,)), dma((2, nz // 2, 2)), dma((2, nz // 2, 2)), dma((nx,)), dma((nx,)), dma((nx,)),
        dma((nx,)), dma((ny,)), dma((ny,)), hops_m, hops_m, hops_h, hops_h, handed_h, handed_h,
    ]
    spec = pl.BlockSpec(memory_space=pltpu.VMEM)
    operands = (
        query_latent, shared_latent, rotary_key.T, *tables, query_gain,
        shared_gain[None], plain_weight, turn_weight.T, key_weight, value_weight, mixer_weight, tokens,
        token_gain[None], routing.T, routing_weight.T, gate[0], up[0], down[0],
    )
    return pl.pallas_call(
        functools.partial(kernel, sizes),
        out_shape=(
            pltpu.VMEM((rows, pieces * LANES), BF16),
            pltpu.VMEM((count_of, pieces * LANES), BF16),
        ),
        in_specs=[spec] * len(operands),
        out_specs=(spec, spec),
        scratch_shapes=scratch,
        compiler_params=pltpu.CompilerParams(
            collective_id=0, has_side_effects=True, vmem_limit_bytes=56 * 1024 * 1024
        ),
        name="step",
    )(*operands)


def build(mesh, nx, cap, spaced):
    nz, ny = mesh.shape["ep"] // nx, mesh.shape["tp"] // 2
    finer = Mesh(mesh.devices.reshape(nz, nx, ny, 2), ("z", "x", "y", "c"))
    placed = (
        P(EP, None), P(EP, None), P(EP, None), P(), P(), P(None, TP), P(None, TP), P(None, TP), P(None, TP),
        P(TP, None), P(EP, None), P(), P(EP, None), P(EP, None), P(EP, None, TP), P(EP, None, TP), P(EP, TP, None),
    )
    return jax.shard_map(
        functools.partial(per_device, (nz, nx, ny, cap, spaced)),
        mesh=finer, in_specs=placed, out_specs=(P(EP, None), P(EP, None)), check_vma=False,
    )


def solution(mesh):
    return build(mesh, NX, 21, 24)
```

```python
import functools
import math

import jax
import jax.numpy as jnp
import numpy as np
from jax import lax
from jax.experimental import pallas as pl
from jax.experimental.pallas import tpu as pltpu
from jax.sharding import Mesh
from jax.sharding import PartitionSpec as P

MESH = pl.DeviceIdType.MESH
F32 = jnp.float32
BF16 = jnp.bfloat16
NOPE = 128
ROPE = 64
LANES = 128
EPSILON = 1e-06
CLAMP_LIMIT = 7.0
SLOPE = 1.702
ROTARY_BASE = 10000.0
NEGATIVE = -1e30
EP = ("z", "x")
TP = ("y", "c")
NX = 4
PARTS = 4
COUNT_IN = 21
CLOCK = {
    "start": 0.1, "arrive": 7.0, "gather": (9.5, 4.5, 3.8), "scatter": (27.0, 4.0, 4.0), "back": 53.0,
    "last": 54.0, "keys": (1.0, 9.2, 6.3), "queries": 11.0, "attend": (11.5, 6.4), "merge": 33.5, "mixer": 34.0,
    "mixer_gather": 48.0,
}


def dot(a, b, on_a=1, on_b=0):
    return lax.dot_general(a, b, (((on_a,), (on_b,)), ((), ())), preferred_element_type=F32)


def iota(shape, dim):
    return lax.broadcasted_iota(jnp.int32, shape, dim)


def normed(ref, gain_ref):
    wide = ref[...].astype(F32)
    wide = wide * lax.rsqrt(jnp.mean(wide * wide, axis=-1, keepdims=True) + EPSILON)
    return (wide * gain_ref[...]).astype(BF16)


def turned(u, cosine, sine):
    half = u.shape[0] // 2
    lower, upper = u[:half], u[half:]
    return jnp.concatenate([lower * cosine - upper * sine, upper * cosine + lower * sine], axis=0)


class Sender:
    def __init__(self):
        self.owed = []

    def copy(self, src, dst, send_sem, recv_sem, device):
        return pltpu.make_async_remote_copy(
            src_ref=src, dst_ref=dst, send_sem=send_sem, recv_sem=recv_sem,
            device_id=device, device_id_type=MESH,
        )

    def start(self, *what):
        made = self.copy(*what)
        made.start()
        self.owed.append(made.wait_send)

    def finish(self):
        for wait in self.owed:
            wait()


def cuts(rows, parts):
    edges = [rows * i // parts // 16 * 16 for i in range(parts)] + [rows]
    return [(lo, hi - lo) for lo, hi in zip(edges, edges[1:])]


def in_order(parts):
    return [[(i + half * parts // 2, way) for half in range(2) for way in range(2)] for i in range(parts // 2)]


def ring_gather(send, axis, size, piece, rows, parts, send_sem, recv_sem, clock, pair=None, far=True):
    me = lax.axis_index(axis)
    ways = ({axis: lax.rem(me + 1, size)}, {axis: lax.rem(me + size - 1, size)})
    steps = size // 2 if far else size // 2 - 1
    start, first, period = clock

    def part(offset, i):
        return piece(lax.rem(me + offset + size, size), *cuts(rows, parts)[i])

    def in_use(step, way, i):
        return step <= steps and (2 * step < size or way == 2 * i // parts)

    def hop(step, way, i):
        ref = part((1 - step) if way == 0 else (step - 1), i)
        at = (way, step - 1, i)
        return (ref, ref, send_sem.at[at], recv_sem.at[at], ways[way])

    def hand(ref, at):
        if pair is not None:
            device, pair_send, pair_recv = pair
            send.start(ref, ref, pair_send.at[at], pair_recv.at[at], device)

    for group in in_order(parts):
        for i, way in group:
            if in_use(1, way, i):
                send.start(*hop(1, way, i))
    if pair is not None:
        for i in range(parts):
            hand(part(0, i), (0, size // 2, i))
    for step in range(1, steps + 1):
        for g, group in enumerate(in_order(parts)):
            yield (step, start + first + period * (step - 1 + 2 * g / parts))
            for i, way in group:
                if in_use(step, way, i):
                    at = (way, step - 1, i)
                    ref = part(-step if way == 0 else step, i)
                    send.copy(ref, ref, send_sem.at[at], recv_sem.at[at], ways[way]).wait_recv()
                    if in_use(step + 1, way, i):
                        send.start(*hop(step + 1, way, i))
                    hand(ref, at)


def pair_arrived(send, size, axis, piece, rows, parts, step, pair):
    device, pair_send, pair_recv = pair
    me = lax.axis_index(axis)
    steps = size // 2
    if step == 0:
        todo = [((0, steps, i), 0, i) for i in range(parts)]
    else:
        todo = [
            ((way, step - 1, i), -step if way == 0 else step, i)
            for i in range(parts) for way in range(2) if step < steps or way == 2 * i // parts
        ]
    for at, offset, i in todo:
        ref = piece(lax.rem(me + offset + size, size), *cuts(rows, parts)[i])
        send.copy(ref, ref, pair_send.at[at], pair_recv.at[at], device).wait_recv()


def near_gather(send, piece, piece_other, rows, sems, device, start):
    send_sem, recv_sem, pair_send, pair_recv = sems
    size, half = 8, rows // 2
    me = lax.axis_index("y")

    def at_piece(offset):
        return lax.rem(me + offset + size, size)

    def span(k, way):
        return (way * half, half) if k == 3 else (0, rows)

    def copy(k, way, source, to):
        ref = piece(at_piece(source), *span(k, way))
        return (ref, ref, send_sem.at[way, k], recv_sem.at[way, k], {"y": at_piece(to)})

    def hand(which, at, offset, lo, count):
        ref = which(at_piece(offset), lo, count)
        return (ref, ref, pair_send.at[at], pair_recv.at[at], device)

    signs = (1, -1)
    for k, distance in ((1, 2), (0, 1)):
        for way, sign in enumerate(signs):
            send.start(*copy(k, way, 0, sign * distance))
    send.start(*hand(piece, (0, 4), 0, 0, rows))
    for k, distance in ((1, 2), (0, 1), (2, 3), (3, 4)):
        yield start + (4.0, 4.0, 7.0, 8.0)[distance - 1]
        for way, sign in enumerate(signs):
            send.copy(*copy(k, way, -sign * distance, 0)).wait_recv()
            if k == 1:
                send.start(*copy(3, way, -sign * 2, sign * 2))
                send.start(*copy(2, way, -sign * 2, sign))
            send.start(*hand(piece, (way, k), -sign * distance, *span(k, way)))
    yield start + 9.0
    send.copy(*hand(piece_other, (0, 4), 0, 0, rows)).wait_recv()
    for k, distance in ((1, 2), (0, 1), (2, 3), (3, 4)):
        for way, sign in enumerate(signs):
            send.copy(*hand(piece_other, (way, k), -sign * distance, *span(k, way))).wait_recv()


class PairSum:
    def __init__(self, send, size, product, part, given, sems, device):
        self.send, self.size, self.product, self.part, self.given = send, size, product, part, given
        self.sems, self.device = sems, device
        self.me, self.core = lax.axis_index("y"), lax.axis_index("c")
        self.seen = set()

    def at(self, offset):
        return lax.rem(self.me + offset + self.size, self.size)

    def copy(self, offset):
        p, i = self.at(offset), offset % self.size
        pair_send, pair_recv = self.sems
        return (self.part.at[1 - self.core, p], self.given.at[p], pair_send.at[i], pair_recv.at[i], self.device)

    def make(self, *offsets):
        for offset in offsets:
            p = self.at(offset)
            both = self.product(p).astype(BF16)
            self.part[0, p] = both[:, :LANES]
            self.part[1, p] = both[:, LANES:]
            self.send.start(*self.copy(offset))

    def own(self, offset, where):
        if offset % self.size not in self.seen:
            self.seen.add(offset % self.size)
            self.send.copy(*self.copy(offset)).wait_recv()
        p = self.at(offset)
        return self.part[self.core, p, where].astype(F32) + self.given[p, where].astype(F32)

    def emit(self, offset, where, value, *to):
        self.part[self.core, self.at(offset), where] = value.astype(BF16)
        self.send.start(self.part.at[self.core, self.at(offset), where], *to)


def ring_scatter(send, size, sums, ring, parts, sems, result, clock):
    send_sem, recv_sem = sems
    me = lax.axis_index("y")
    ways = ({"y": lax.rem(me + 1, size)}, {"y": lax.rem(me + size - 1, size)})
    steps = size // 2
    spans = [pl.ds(*cut) for cut in cuts(ring.shape[2], parts)]

    def in_use(step, way, i):
        return step >= 2 or way == 2 * i // parts

    def arrival(step, way, i):
        at = (way, step - 1, i)
        ref = ring.at[way, step - 1, spans[i]]
        send.copy(ref, ref, send_sem.at[at], recv_sem.at[at], ways[way]).wait_recv()
        return ring[way, step - 1, spans[i]].astype(F32)

    start, first, period = clock
    sums.make(steps)
    if steps > 1:
        sums.make(steps - 1, 1 - steps)
    for step in range(1, steps + 1):
        for g, group in enumerate(in_order(parts)):
            yield start + (first + period * (step - 2 + 2 * g / parts) if step > 1 else 0.0)
            for i, way in group:
                if in_use(step, way, i):
                    offset = (steps - step + 1) * (1 if way == 0 else -1)
                    value = sums.own(offset, spans[i])
                    if step > 1 and in_use(step - 1, way, i):
                        value = value + arrival(step - 1, way, i)
                    at = (way, step - 1, i)
                    sums.emit(
                        offset, spans[i], value, ring.at[way, step - 1, spans[i]],
                        send_sem.at[at], recv_sem.at[at], ways[way],
                    )
        if steps - step > 1:
            sums.make(steps - step - 1, 1 + step - steps)
        elif steps - step == 1 or steps == 1:
            sums.make(0)
    yield start + first + period * (steps - 0.5)
    for i in range(parts):
        value = sums.own(0, spans[i])
        for way in range(2):
            if in_use(steps, way, i):
                value = value + arrival(steps, way, i)
        result[spans[i]] = value.astype(BF16)


def near_scatter(send, sums, held, sems, result, start):
    send_sem, recv_sem = sems
    rows = held.shape[2]
    whole = pl.ds(0, rows)

    def span(k, way):
        return pl.ds(way * (rows // 2), rows // 2) if k == 1 else whole

    def to(k, way, distance):
        sign = 1 - 2 * way
        return (
            held.at[way, k, span(k, way)], send_sem.at[way, k], recv_sem.at[way, k],
            {"y": sums.at(sign * distance)},
        )

    def arrival(k, way):
        ref = held.at[way, k, span(k, way)]
        send.copy(ref, *to(k, way, 1)).wait_recv()
        return held[way, k, span(k, way)].astype(F32)

    sums.make(4, 3, -3)
    yield start + 1.0
    sums.make(2, -2, 1, -1, 0)
    yield start + 2.0
    for way, sign in enumerate((1, -1)):
        sums.emit(4 * sign, span(1, way), sums.own(4 * sign, span(1, way)), *to(1, way, 2))
    for way, sign in enumerate((1, -1)):
        sums.emit(3 * sign, whole, sums.own(3 * sign, whole), *to(0, way, 1))
    yield start + 8.0
    for way, sign in enumerate((1, -1)):
        value = sums.own(2 * sign, whole) + arrival(0, way)
        far = arrival(1, way)
        pad = jnp.zeros_like(far)
        value = value + jnp.concatenate([far, pad] if way == 0 else [pad, far], axis=0)
        sums.emit(2 * sign, whole, value, *to(3, way, 2))
    for way, sign in enumerate((1, -1)):
        sums.emit(sign, whole, sums.own(sign, whole), *to(2, way, 1))
    yield start + 14.0
    value = sums.own(0, whole)
    for k in (2, 3):
        for way in range(2):
            value = value + arrival(k, way)
    result[...] = value.astype(BF16)


def exchange(send, nz, nx, src, dst, send_sem, recv_sem):
    count = nz * nx
    me = lax.axis_index("z") * nx + lax.axis_index("x")

    def out(d):
        to = lax.rem(me + d, count)
        return send.copy(
            src.at[to], dst.at[me], send_sem.at[d], recv_sem.at[d], {"z": to // nx, "x": lax.rem(to, nx)}
        )

    @pl.loop(1, count)
    def _(d):
        out(d).start()

    def wait():
        @pl.loop(1, count)
        def _(d):
            origin = lax.rem(me + count - d, count)
            send.copy(
                src.at[origin], dst.at[origin], send_sem.at[d], recv_sem.at[d],
                {"z": origin // nx, "x": lax.rem(origin, nx)},
            ).wait_recv()

    def sent():
        @pl.loop(1, count)
        def _(d):
            out(d).wait_send()

    send.owed.append(sent)
    dst[me] = src[me]
    return wait


def kernel(sizes, *refs):
    nz, nx, ny, cap, spaced = sizes
    given, (mixer_out, expert_out) = refs[:COUNT_IN], refs[COUNT_IN : COUNT_IN + 2]
    inputs, scratch = refs[COUNT_IN + 2 : 2 * COUNT_IN + 2], refs[2 * COUNT_IN + 2 :]
    (routing, routing_weight, tokens, token_gain, query_latent, shared_latent, rotary_key, inside_cos, inside_sin,
     block_cos, block_sin, query_gain, shared_gain, plain_weight, turn_weight, key_weight, value_weight,
     gate, up, down, mixer_weight) = inputs
    (out_rows, in_rows, out_far, in_far, pack, mix_high, mix_low, gath, gate_up, hidden, part_e, given_e, ring_e,
     back_out, back_in, result_e, queries, query_1, query_2, keys, peak, total, accum, share_out, stat_out, share_in,
     stat_in, heads, part_m, given_m, ring_m,
     s_in, s_a, r_a, s_x, r_x, sp_x, rp_x, s_g, r_g, sp_g, rp_g, sp_e, rp_e, s_e, r_e, s_b, r_b, s_f, r_f, sp_f, rp_f,
     s_q, r_q, s_k, r_k, s_o, r_o, s_t, r_t, sp_m, rp_m, s_m, r_m, s_h, r_h, sp_h, rp_h) = scratch
    z, x, y, core = (lax.axis_index(a) for a in ("z", "x", "y", "c"))
    count = nz * nx
    me = z * nx + x
    turn = 2 * y + core
    rows = query_latent.shape[0]
    other = {"c": 1 - core}
    send = Sender()

    barrier = pltpu.get_barrier_semaphore()

    @pl.loop(1, count)
    def _(d):
        to = lax.rem(me + d, count)
        pl.semaphore_signal(
            barrier, inc=1, device_id={"z": to // nx, "x": lax.rem(to, nx)}, device_id_type=MESH
        )

    greeted = [{"y": lax.rem(y + d + ny, ny)} for d in ((1, -1, 2, -2) if ny == 8 else (1, -1))] + [other]
    for device in greeted:
        pl.semaphore_signal(barrier, inc=1, device_id=device, device_id_type=MESH)

    loads = [pltpu.make_async_copy(a, b, s_in.at[i]) for i, (a, b) in enumerate(zip(given, inputs))]
    for load in loads:
        load.start()

    def loaded(first, last):
        for load in loads[first:last]:
            load.wait()

    def gather_columns(ref, sems, start):
        def piece(p, lo, size):
            return ref.at[pl.ds(lo, size), pl.ds(pl.multiple_of((2 * p + core) * LANES, LANES), LANES)]

        def piece_other(p, lo, size):
            return ref.at[pl.ds(lo, size), pl.ds(pl.multiple_of((2 * p + 1 - core) * LANES, LANES), LANES)]

        if ny == 8:
            yield from near_gather(send, piece, piece_other, ref.shape[0], sems, other, start)
        else:
            pair = (other, *sems[2:])
            for _, when in ring_gather(send, "y", ny, piece, ref.shape[0], 2, *sems[:2], (start, 4.0, 4.0), pair):
                yield when
            for step in range(ny // 2 + 1):
                pair_arrived(send, ny, "y", piece_other, ref.shape[0], 2, step, pair)

    def expert_chain():
        width = pl.ds(pl.multiple_of(turn * LANES, LANES), LANES)
        far = lax.rem(y + ny // 2, ny)
        far_width = pl.ds(pl.multiple_of((2 * far + core) * LANES, LANES), LANES)
        loaded(0, 4)
        wide = tokens[...].astype(F32)
        factor = lax.rsqrt(jnp.mean(wide * wide, axis=-1, keepdims=True) + EPSILON)
        own, own_far = (
            (tokens[:, w].astype(F32) * factor * token_gain[:, w]).astype(BF16) for w in (width, far_width)
        )
        count_of = own.shape[0]
        named = iota((count, count_of), 0)
        member = jnp.zeros((count, count_of), F32)
        weight = jnp.zeros((count, count_of), F32)
        for k in range(routing.shape[0]):
            hit = routing[k : k + 1, :] == named
            member = member + jnp.where(hit, 1.0, 0.0)
            weight = weight + jnp.where(hit, routing_weight[k : k + 1, :], 0.0)
        member = member.astype(BF16)
        earlier = jnp.where(
            iota((count_of, count_of), 0) < iota((count_of, count_of), 1), 1.0, 0.0
        ).astype(BF16)
        rank = dot(member, earlier).astype(BF16)
        slots = count * spaced

        def block(line):
            return ((line.astype(F32) + 0.5) * (1.0 / spaced)).astype(jnp.int32)

        spread = jnp.where(block(iota((slots, count), 0)) == iota((slots, count), 1), 1.0, 0.0).astype(BF16)
        line = iota((slots, count_of), 0)
        place = (line - block(line) * spaced).astype(F32)
        chosen = (dot(spread, member) > 0.5) & (dot(spread, rank) == place)
        high = weight.astype(BF16)
        low = (weight - high.astype(F32)).astype(BF16)
        mix_high[...] = jnp.where(chosen, dot(spread, high), 0.0).astype(BF16)
        mix_low[...] = jnp.where(chosen, dot(spread, low), 0.0).astype(BF16)
        chosen = jnp.where(chosen, 1.0, 0.0).astype(BF16)
        out_rows[...] = dot(chosen, own).astype(BF16).reshape(out_rows.shape)
        out_far[...] = dot(chosen, own_far).astype(BF16).reshape(out_far.shape)
        yield 0.0
        arrive = exchange(send, nz, nx, out_rows, in_rows, s_a, r_a)
        column = iota(pack.shape, 1)
        inner = column - block(column) * spaced
        goal = jnp.where(inner < cap, block(column) * cap + inner, -1)
        pack[...] = jnp.where(goal == iota(pack.shape, 0), 1.0, 0.0).astype(BF16)
        gate_up[...] = jnp.zeros_like(gate_up)
        yield CLOCK["arrive"]
        arrive()
        gath[turn] = dot(pack[...], in_rows[...].reshape(slots, LANES)).astype(BF16)
        slot = lambda p: 2 * p + core
        slot_other = lambda p: 2 * p + 1 - core
        packed = gath.shape[1]
        piece = lambda p, lo, size: gath.at[slot(p), pl.ds(lo, size)]
        piece_other = lambda p, lo, size: gath.at[slot_other(p), pl.ds(lo, size)]
        pair = (other, sp_g, rp_g)
        ring = ring_gather(send, "y", ny, piece, packed, PARTS, s_g, r_g, CLOCK["gather"], pair, False)
        ahead = next(ring, None)
        arrive_far = exchange(send, nz, nx, out_far, in_far, s_x, r_x)

        def consume(piece):
            rows_of = pl.ds(pl.multiple_of(piece * LANES, LANES), LANES)
            both = jnp.concatenate([gate[rows_of, :], up[rows_of, :]], axis=1)
            gate_up[...] += dot(gath[piece], both)

        def consume_step(step, which):
            for offset in sorted({-step % ny, step % ny}):
                consume(which(lax.rem(y + offset, ny)))

        far_slot, far_other = slot(far), slot_other(far)
        far_copy = (gath.at[far_slot], gath.at[far_slot], sp_x, rp_x, other)
        loaded(17, 19)
        consume_step(0, slot)
        for step in range(1, ny // 2 + 1):
            behind = step - 1
            while ahead is not None and ahead[0] == step:
                yield ahead[1]
                ahead = next(ring, None)
                if behind is not None:
                    pair_arrived(send, ny, "y", piece_other, packed, PARTS, behind, pair)
                    consume_step(behind, slot_other)
                    behind = None
            if behind is not None:
                pair_arrived(send, ny, "y", piece_other, packed, PARTS, behind, pair)
                consume_step(behind, slot_other)
            if step == max(1, ny // 2 - 2):
                arrive_far()
                gath[far_slot] = dot(pack[...], in_far[...].reshape(slots, LANES)).astype(BF16)
                send.start(*far_copy)
                consume(far_slot)
            if step < ny // 2:
                consume_step(step, slot)
        ref = gath.at[far_other]
        send.copy(ref, ref, sp_x, rp_x, other).wait_recv()
        consume(far_other)
        gate_pre = jnp.minimum(gate_up[:, :LANES], CLAMP_LIMIT)
        up_pre = jnp.clip(gate_up[:, LANES:], -CLAMP_LIMIT, CLAMP_LIMIT)
        hidden[...] = ((up_pre + 1.0) * (gate_pre * jax.nn.sigmoid(SLOPE * gate_pre))).astype(BF16)

        def product(p):
            return dot(hidden[...], down[:, pl.ds(pl.multiple_of(2 * LANES * p, 2 * LANES), 2 * LANES)])

        loaded(19, 20)
        sums = PairSum(send, ny, product, part_e, given_e, (sp_e, rp_e), other)
        yield from ring_scatter(send, ny, sums, ring_e, PARTS, (s_e, r_e), result_e, CLOCK["scatter"])
        back_out[...] = dot(pack[...], result_e[...], 0, 0).astype(BF16).reshape(back_out.shape)
        arrive = exchange(send, nz, nx, back_out, back_in, s_b, r_b)
        yield CLOCK["back"]
        arrive()
        back = back_in[...].reshape(slots, LANES)
        mixed = dot(mix_high[...], back, 0, 0) + dot(mix_low[...], back, 0, 0)
        expert_out[:, width] = mixed.astype(BF16)
        yield from gather_columns(expert_out, (s_f, r_f, sp_f, rp_f), CLOCK["last"])

    def mixer_chain():
        scale = (NOPE + ROPE) ** -0.5 * math.log2(math.e)
        loaded(4, 17)
        mine = iota(block_cos.shape, 1) == me
        cos_b = jnp.sum(jnp.where(mine, block_cos[...], 0.0), axis=1, keepdims=True)
        sin_b = jnp.sum(jnp.where(mine, block_sin[...], 0.0), axis=1, keepdims=True)
        cosine = inside_cos[...] * cos_b - inside_sin[...] * sin_b
        sine = inside_sin[...] * cos_b + inside_cos[...] * sin_b
        latent = normed(query_latent, query_gain)
        queries[x, :rows] = dot(latent, plain_weight[...]).astype(BF16)
        raw = turned(dot(turn_weight[...], latent, 1, 1), cosine, sine)
        raw = jnp.concatenate([raw, jnp.zeros_like(raw)], axis=0)
        queries[x, rows:] = raw.T.astype(BF16)
        shared = normed(shared_latent, shared_gain)
        keys[z, :rows] = dot(shared, key_weight[...]).astype(BF16)
        keys[z, rows : 2 * rows] = dot(shared, value_weight[...]).astype(BF16)
        raw = turned(rotary_key[...].astype(F32), cosine, sine)
        raw = jnp.concatenate([raw[:, : rows // 2], raw[:, rows // 2 :]], axis=0)
        keys[z, 2 * rows :] = raw.T.astype(BF16)
        yield CLOCK["start"]
        keys_here.append(ring_gather(
            send, "z", nz, lambda p, lo, size: keys.at[p, pl.ds(lo, size)], keys.shape[1], 2, s_k, r_k, CLOCK["keys"]
        ))
        ahead.append(next(keys_here[0], None))
        to_x = [lax.rem(x + d, nx) for d in range(nx)]
        from_x = [lax.rem(x + nx - d, nx) for d in range(nx)]
        for d in range(1, nx):
            send.start(queries.at[x], queries.at[x], s_q.at[d], r_q.at[d], {"x": to_x[d]})
        yield CLOCK["queries"]
        for d in range(1, nx):
            ref = queries.at[from_x[d]]
            send.copy(ref, ref, s_q.at[d], r_q.at[d], {"x": to_x[d]}).wait_recv()
        move = jnp.where(iota((LANES, LANES), 0) + ROPE == iota((LANES, LANES), 1), 1.0, 0.0).astype(BF16)
        for j in range(nx):
            span = pl.ds(j * rows, rows)
            plain, turned_part = queries[j, :rows], queries[j, rows:]
            query_1[span, :LANES] = plain
            query_1[span, LANES:] = turned_part
            query_2[span, :LANES] = plain
            query_2[span, LANES:] = dot(turned_part, move).astype(BF16)

        def attend(piece, own):
            half = rows // 2
            both = keys[piece, 2 * rows :]
            key_1 = jnp.concatenate([keys[piece, :half], both], axis=1)
            key_2 = jnp.concatenate([keys[piece, half:rows], both], axis=1)
            scores = jnp.concatenate(
                [dot(key_1, query_1[...], 1, 1), dot(key_2, query_2[...], 1, 1)], axis=0
            )
            if own:
                visible = iota(scores.shape, 0) + rows * x <= iota(scores.shape, 1)
                scores = jnp.where(visible, scores, NEGATIVE)
            highest = jnp.max(scores, axis=0, keepdims=True)
            if not own:
                highest = jnp.maximum(highest, peak[...])
            probs = jnp.exp2((scores - highest) * scale)
            summed = jnp.sum(probs, axis=0, keepdims=True)
            mixed = dot(keys[piece, rows : 2 * rows], probs.astype(BF16), 0, 0)
            if own:
                total[...] = summed
                accum[...] = mixed
            else:
                fade = jnp.exp2((peak[...] - highest) * scale)
                total[...] = total[...] * fade + summed
                accum[...] = accum[...] * fade + mixed
            peak[...] = highest

        attend(z, True)
        steps = nz // 2
        for step in range(1, steps + 1):
            yield CLOCK["attend"][0] + CLOCK["attend"][1] * (step - 1)
            while ahead[0] is not None and ahead[0][0] == step:
                ahead[0] = next(keys_here[0], None)

            @pl.when(z >= step)
            def _():
                attend(lax.rem(z - step + nz, nz), False)

            if step < steps:
                @pl.when(z + step >= nz)
                def _():
                    attend(lax.rem(z + step, nz), False)

        share = (accum[...] / total[...]).astype(BF16)
        for j in range(nx):
            span = slice(j * rows, (j + 1) * rows)
            share_out[j] = share[:, span]
            stat = (8, rows)
            stat_out[j] = jnp.where(iota(stat, 0) == 0, peak[:, span], total[:, span])
        for d in range(1, nx):
            device = {"x": to_x[d]}
            send.start(share_out.at[to_x[d]], share_in.at[x], s_o.at[d], r_o.at[d], device)
            send.start(stat_out.at[to_x[d]], stat_in.at[x], s_t.at[d], r_t.at[d], device)
        share_in[x] = share_out[x]
        stat_in[x] = stat_out[x]
        yield CLOCK["merge"]
        for d in range(1, nx):
            device = {"x": to_x[d]}
            for ref, s, r in ((share_in, s_o, r_o), (stat_in, s_t, r_t)):
                ref = ref.at[from_x[d]]
                send.copy(ref, ref, s.at[d], r.at[d], device).wait_recv()
        peaks = [stat_in[j, 0:1, :] for j in range(nx)]
        highest = functools.reduce(jnp.maximum, peaks)
        factors = [stat_in[j, 1:2, :] * jnp.exp2((peaks[j] - highest) * scale) for j in range(nx)]
        merged = sum(share_in[j].astype(F32) * factors[j] for j in range(nx)) / sum(factors)
        heads[...] = merged.astype(BF16)

        def product(p):
            columns = pl.ds(pl.multiple_of(2 * LANES * p, 2 * LANES), 2 * LANES)
            return dot(heads[...], mixer_weight[:, columns], 0, 0)

        loaded(20, 21)
        yield CLOCK["mixer"]
        sums = PairSum(send, ny, product, part_m, given_m, (sp_m, rp_m), other)
        result = mixer_out.at[:, pl.ds(pl.multiple_of(turn * LANES, LANES), LANES)]
        if ny == 8:
            yield from near_scatter(send, sums, ring_m, (s_m, r_m), result, CLOCK["mixer"])
        else:
            yield from ring_scatter(send, ny, sums, ring_m, 2, (s_m, r_m), result, (CLOCK["mixer"], 3.5, 3.5))
        yield from gather_columns(mixer_out, (s_h, r_h, sp_h, rp_h), CLOCK["mixer_gather"])

    keys_here, ahead = [], []

    def keys_chain():
        yield CLOCK["keys"][0] + CLOCK["keys"][1]
        while ahead[0] is not None:
            ahead[0] = next(keys_here[0], None)
            if ahead[0] is not None:
                yield ahead[0][1]

    chains = [expert_chain(), keys_chain(), mixer_chain()]
    waiting = [(next(chain), i) for i, chain in enumerate(chains)]
    pl.semaphore_wait(barrier, count - 1 + len(greeted))
    while waiting:
        _, i = waiting.pop(waiting.index(min(waiting)))
        when = next(chains[i], None)
        if when is not None:
            waiting.append((when, i))
    send.finish()


def per_device(sizes, query_latent, shared_latent, rotary_key, query_gain, shared_gain, plain_weight, turn_weight,
               key_weight, value_weight, mixer_weight, tokens, token_gain, routing, routing_weight, gate, up, down):
    nz, nx, ny, cap, spaced = sizes
    rows = query_latent.shape[0]
    count, pieces = nz * nx, 2 * ny
    frequency = ROTARY_BASE ** (-2.0 * np.arange(ROPE // 2) / ROPE)
    inside = frequency[:, None] * np.arange(rows)
    blocks = frequency[:, None] * (np.arange(count) * rows)
    tables = [jnp.asarray(f(a), F32) for a in (inside, blocks) for f in (np.cos, np.sin)]
    slots, packed = count * spaced, count * cap
    count_of = tokens.shape[0]
    vmem, dma = pltpu.VMEM, pltpu.SemaphoreType.DMA
    hops, handed = dma((2, ny // 2, PARTS)), dma((2, ny // 2 + 1, PARTS))
    if ny == 8:
        hops_m, hops_h, handed_h = dma((2, 4)), dma((2, 4)), dma((2, 5))
    else:
        hops_m, hops_h, handed_h = hops, hops, handed
    scratch = [
        vmem((count, spaced, LANES), BF16), vmem((count, spaced, LANES), BF16),
        vmem((count, spaced, LANES), BF16), vmem((count, spaced, LANES), BF16), vmem((packed, slots), BF16),
        vmem((slots, count_of), BF16), vmem((slots, count_of), BF16), vmem((pieces, packed, LANES), BF16),
        vmem((packed, 2 * LANES), F32), vmem((packed, LANES), BF16), vmem((2, ny, packed, LANES), BF16),
        vmem((ny, packed, LANES), BF16), vmem((2, ny // 2, packed, LANES), BF16),
        vmem((count, spaced, LANES), BF16), vmem((count, spaced, LANES), BF16), vmem((packed, LANES), BF16),
        vmem((nx, 2 * rows, LANES), BF16), vmem((nx * rows, 2 * LANES), BF16), vmem((nx * rows, 2 * LANES), BF16),
        vmem((nz, 2 * rows + rows // 2, LANES), BF16), vmem((1, nx * rows), F32), vmem((1, nx * rows), F32),
        vmem((LANES, nx * rows), F32), vmem((nx, LANES, rows), BF16), vmem((nx, 8, rows), F32),
        vmem((nx, LANES, rows), BF16), vmem((nx, 8, rows), F32), vmem((LANES, rows), BF16),
        vmem((2, ny, rows, LANES), BF16), vmem((ny, rows, LANES), BF16), vmem((2, ny // 2, rows, LANES), BF16),
        dma((COUNT_IN,)), dma((count,)), dma((count,)), dma((count,)), dma((count,)), dma, dma,
        hops, hops, handed, handed, dma((ny,)), dma((ny,)), hops, hops,
        dma((count,)), dma((count,)), hops_h, hops_h, handed_h, handed_h,
        dma((nx,)), dma((nx,)), dma((2, nz // 2, 2)), dma((2, nz // 2, 2)), dma((nx,)), dma((nx,)), dma((nx,)),
        dma((nx,)), dma((ny,)), dma((ny,)), hops_m, hops_m, hops_h, hops_h, handed_h, handed_h,
    ]
    spec = pl.BlockSpec(memory_space=pltpu.VMEM)
    operands = (
        routing.T, routing_weight.T, tokens, token_gain[None], query_latent, shared_latent, rotary_key.T, *tables,
        query_gain, shared_gain[None], plain_weight, turn_weight.T, key_weight, value_weight,
        gate[0], up[0], down[0], mixer_weight,
    )
    scratch = [vmem(a.shape, a.dtype) for a in operands] + scratch
    return pl.pallas_call(
        functools.partial(kernel, sizes),
        out_shape=(
            pltpu.VMEM((rows, pieces * LANES), BF16),
            pltpu.VMEM((count_of, pieces * LANES), BF16),
        ),
        in_specs=[pl.BlockSpec(memory_space=pltpu.HBM)] * len(operands),
        out_specs=(spec, spec),
        scratch_shapes=scratch,
        compiler_params=pltpu.CompilerParams(
            collective_id=0, has_side_effects=True, vmem_limit_bytes=56 * 1024 * 1024
        ),
        name="step",
    )(*operands)


def build(mesh, nx, cap, spaced):
    nz, ny = mesh.shape["ep"] // nx, mesh.shape["tp"] // 2
    finer = Mesh(mesh.devices.reshape(nz, nx, ny, 2), ("z", "x", "y", "c"))
    placed = (
        P(EP, None), P(EP, None), P(EP, None), P(), P(), P(None, TP), P(None, TP), P(None, TP), P(None, TP),
        P(TP, None), P(EP, None), P(), P(EP, None), P(EP, None), P(EP, None, TP), P(EP, None, TP), P(EP, TP, None),
    )
    return jax.shard_map(
        functools.partial(per_device, (nz, nx, ny, cap, spaced)),
        mesh=finer, in_specs=placed, out_specs=(P(EP, None), P(EP, None)), check_vma=False,
    )


def solution(mesh):
    return build(mesh, NX, 21, 24)
```

```python
import functools
import math

import jax
import jax.numpy as jnp
import numpy as np
from jax import lax
from jax.experimental import pallas as pl
from jax.experimental.pallas import tpu as pltpu
from jax.sharding import Mesh
from jax.sharding import PartitionSpec as P

MESH = pl.DeviceIdType.MESH
F32 = jnp.float32
BF16 = jnp.bfloat16
NOPE = 128
ROPE = 64
LANES = 128
EPSILON = 1e-06
CLAMP_LIMIT = 7.0
SLOPE = 1.702
ROTARY_BASE = 10000.0
NEGATIVE = -1e30
EP = ("z", "x")
TP = ("y", "c")
NX = 4
PARTS = 4
COUNT_IN = 21
CLOCK = {
    "local": 0.05, "more": 0.2, "start": 0.1, "arrive": 7.0, "gather": (9.5, 4.5, 3.8), "scatter": (27.0, 4.0, 4.0), "back": 54.8,
    "last": 55.5, "keys": (1.0, (10.2, 18.7, 22.9, 26.5), None), "queries": 11.0, "attend": (11.9, 18.9, 23.0, 29.0), "merge": 35.2, "mixer": 36.0, "mid": 44.0, "end": 50.0,
    "mixer_gather": 50.5,
}


def dot(a, b, on_a=1, on_b=0):
    return lax.dot_general(a, b, (((on_a,), (on_b,)), ((), ())), preferred_element_type=F32)


def iota(shape, dim):
    return lax.broadcasted_iota(jnp.int32, shape, dim)


def normed(ref, gain_ref):
    wide = ref[...].astype(F32)
    wide = wide * lax.rsqrt(jnp.mean(wide * wide, axis=-1, keepdims=True) + EPSILON)
    return (wide * gain_ref[...]).astype(BF16)


def turned(u, cosine, sine):
    half = u.shape[0] // 2
    lower, upper = u[:half], u[half:]
    return jnp.concatenate([lower * cosine - upper * sine, upper * cosine + lower * sine], axis=0)


class Sender:
    def __init__(self):
        self.owed = []

    def copy(self, src, dst, send_sem, recv_sem, device):
        return pltpu.make_async_remote_copy(
            src_ref=src, dst_ref=dst, send_sem=send_sem, recv_sem=recv_sem,
            device_id=device, device_id_type=MESH,
        )

    def start(self, *what):
        made = self.copy(*what)
        made.start()
        self.owed.append(made.wait_send)

    def finish(self, count=None):
        now, self.owed = self.owed[:count], self.owed[len(self.owed[:count]) :]
        for wait in now:
            wait()


def cuts(rows, parts):
    edges = [rows * i // parts // 16 * 16 for i in range(parts)] + [rows]
    return [(lo, hi - lo) for lo, hi in zip(edges, edges[1:])]


def in_order(parts):
    return [[(i + half * parts // 2, way) for half in range(2) for way in range(2)] for i in range(parts // 2)]


def ring_gather(send, axis, size, piece, rows, parts, send_sem, recv_sem, clock, pair=None, far=True):
    me = lax.axis_index(axis)
    ways = ({axis: lax.rem(me + 1, size)}, {axis: lax.rem(me + size - 1, size)})
    steps = size // 2 if far else size // 2 - 1
    start, first, period = clock

    def part(offset, i):
        return piece(lax.rem(me + offset + size, size), *cuts(rows, parts)[i])

    def in_use(step, way, i):
        return step <= steps and (2 * step < size or way == 2 * i // parts)

    def hop(step, way, i):
        ref = part((1 - step) if way == 0 else (step - 1), i)
        at = (way, step - 1, i)
        return (ref, ref, send_sem.at[at], recv_sem.at[at], ways[way])

    def hand(ref, at):
        if pair is not None:
            device, pair_send, pair_recv = pair
            send.start(ref, ref, pair_send.at[at], pair_recv.at[at], device)

    for group in in_order(parts):
        for i, way in group:
            if in_use(1, way, i):
                send.start(*hop(1, way, i))
    if pair is not None:
        for i in range(parts):
            hand(part(0, i), (0, size // 2, i))
    for step in range(1, steps + 1):
        for g, group in enumerate(in_order(parts)):
            yield (step, first[step - 1] if period is None else start + first + period * (step - 1 + 2 * g / parts))
            for i, way in group:
                if in_use(step, way, i):
                    at = (way, step - 1, i)
                    ref = part(-step if way == 0 else step, i)
                    send.copy(ref, ref, send_sem.at[at], recv_sem.at[at], ways[way]).wait_recv()
                    if in_use(step + 1, way, i):
                        send.start(*hop(step + 1, way, i))
                    hand(ref, at)


def pair_arrived(send, size, axis, piece, rows, parts, step, pair):
    device, pair_send, pair_recv = pair
    me = lax.axis_index(axis)
    steps = size // 2
    if step == 0:
        todo = [((0, steps, i), 0, i) for i in range(parts)]
    else:
        todo = [
            ((way, step - 1, i), -step if way == 0 else step, i)
            for i in range(parts) for way in range(2) if step < steps or way == 2 * i // parts
        ]
    for at, offset, i in todo:
        ref = piece(lax.rem(me + offset + size, size), *cuts(rows, parts)[i])
        send.copy(ref, ref, pair_send.at[at], pair_recv.at[at], device).wait_recv()


def near_gather(send, piece, piece_other, rows, sems, device, start):
    send_sem, recv_sem, pair_send, pair_recv = sems
    size, half = 8, rows // 2
    me = lax.axis_index("y")

    def at_piece(offset):
        return lax.rem(me + offset + size, size)

    def span(k, way):
        return (way * half, half) if k == 3 else (0, rows)

    def copy(k, way, source, to):
        ref = piece(at_piece(source), *span(k, way))
        return (ref, ref, send_sem.at[way, k], recv_sem.at[way, k], {"y": at_piece(to)})

    def hand(which, at, offset, lo, count):
        ref = which(at_piece(offset), lo, count)
        return (ref, ref, pair_send.at[at], pair_recv.at[at], device)

    signs = (1, -1)
    for k, distance in ((1, 2), (0, 1)):
        for way, sign in enumerate(signs):
            send.start(*copy(k, way, 0, sign * distance))
    send.start(*hand(piece, (0, 4), 0, 0, rows))
    for k, distance in ((1, 2), (0, 1), (2, 3), (3, 4)):
        yield start + (4.0, 4.0, 7.0, 8.0)[distance - 1]
        for way, sign in enumerate(signs):
            send.copy(*copy(k, way, -sign * distance, 0)).wait_recv()
            if k == 1:
                send.start(*copy(3, way, -sign * 2, sign * 2))
                send.start(*copy(2, way, -sign * 2, sign))
            send.start(*hand(piece, (way, k), -sign * distance, *span(k, way)))
    yield start + 9.0
    send.copy(*hand(piece_other, (0, 4), 0, 0, rows)).wait_recv()
    for k, distance in ((1, 2), (0, 1), (2, 3), (3, 4)):
        for way, sign in enumerate(signs):
            send.copy(*hand(piece_other, (way, k), -sign * distance, *span(k, way))).wait_recv()


class PairSum:
    def __init__(self, send, size, product, part, given, sems, device):
        self.send, self.size, self.product, self.part, self.given = send, size, product, part, given
        self.sems, self.device = sems, device
        self.me, self.core = lax.axis_index("y"), lax.axis_index("c")
        self.seen = set()

    def at(self, offset):
        return lax.rem(self.me + offset + self.size, self.size)

    def copy(self, offset):
        p, i = self.at(offset), offset % self.size
        pair_send, pair_recv = self.sems
        return (self.part.at[1 - self.core, p], self.given.at[p], pair_send.at[i], pair_recv.at[i], self.device)

    def make(self, *offsets):
        for offset in offsets:
            p = self.at(offset)
            both = self.product(p).astype(BF16)
            self.part[0, p] = both[:, :LANES]
            self.part[1, p] = both[:, LANES:]
            self.send.start(*self.copy(offset))

    def own(self, offset, where):
        if offset % self.size not in self.seen:
            self.seen.add(offset % self.size)
            self.send.copy(*self.copy(offset)).wait_recv()
        p = self.at(offset)
        return self.part[self.core, p, where].astype(F32) + self.given[p, where].astype(F32)

    def emit(self, offset, where, value, *to):
        self.part[self.core, self.at(offset), where] = value.astype(BF16)
        self.send.start(self.part.at[self.core, self.at(offset), where], *to)


def ring_scatter(send, size, sums, ring, parts, sems, result, clock):
    send_sem, recv_sem = sems
    me = lax.axis_index("y")
    ways = ({"y": lax.rem(me + 1, size)}, {"y": lax.rem(me + size - 1, size)})
    steps = size // 2
    spans = [pl.ds(*cut) for cut in cuts(ring.shape[2], parts)]

    def in_use(step, way, i):
        return step >= 2 or way == 2 * i // parts

    def arrival(step, way, i):
        at = (way, step - 1, i)
        ref = ring.at[way, step - 1, spans[i]]
        send.copy(ref, ref, send_sem.at[at], recv_sem.at[at], ways[way]).wait_recv()
        return ring[way, step - 1, spans[i]].astype(F32)

    start, first, period = clock
    sums.make(steps)
    if steps > 1:
        sums.make(steps - 1, 1 - steps)
    for step in range(1, steps + 1):
        for g, group in enumerate(in_order(parts)):
            yield start + (first + period * (step - 2 + 2 * g / parts) if step > 1 else 0.0)
            for i, way in group:
                if in_use(step, way, i):
                    offset = (steps - step + 1) * (1 if way == 0 else -1)
                    value = sums.own(offset, spans[i])
                    if step > 1 and in_use(step - 1, way, i):
                        value = value + arrival(step - 1, way, i)
                    at = (way, step - 1, i)
                    sums.emit(
                        offset, spans[i], value, ring.at[way, step - 1, spans[i]],
                        send_sem.at[at], recv_sem.at[at], ways[way],
                    )
        if steps - step > 1:
            sums.make(steps - step - 1, 1 + step - steps)
        elif steps - step == 1 or steps == 1:
            sums.make(0)
    yield start + first + period * (steps - 0.5)
    for i in range(parts):
        value = sums.own(0, spans[i])
        for way in range(2):
            if in_use(steps, way, i):
                value = value + arrival(steps, way, i)
        result[spans[i]] = value.astype(BF16)


def near_scatter(send, sums, held, sems, result, start):
    send_sem, recv_sem = sems
    rows = held.shape[2]
    whole = pl.ds(0, rows)

    def span(k, way):
        return pl.ds(way * (rows // 2), rows // 2) if k == 1 else whole

    def to(k, way, distance):
        sign = 1 - 2 * way
        return (
            held.at[way, k, span(k, way)], send_sem.at[way, k], recv_sem.at[way, k],
            {"y": sums.at(sign * distance)},
        )

    def arrival(k, way):
        ref = held.at[way, k, span(k, way)]
        send.copy(ref, *to(k, way, 1)).wait_recv()
        return held[way, k, span(k, way)].astype(F32)

    sums.make(4, 3, -3)
    yield start + 1.0
    sums.make(2, -2, 1, -1, 0)
    yield start + 2.0
    for way, sign in enumerate((1, -1)):
        sums.emit(4 * sign, span(1, way), sums.own(4 * sign, span(1, way)), *to(1, way, 2))
    for way, sign in enumerate((1, -1)):
        sums.emit(3 * sign, whole, sums.own(3 * sign, whole), *to(0, way, 1))
    yield CLOCK["mid"]
    for way, sign in enumerate((1, -1)):
        value = sums.own(2 * sign, whole) + arrival(0, way)
        far = arrival(1, way)
        pad = jnp.zeros_like(far)
        value = value + jnp.concatenate([far, pad] if way == 0 else [pad, far], axis=0)
        sums.emit(2 * sign, whole, value, *to(3, way, 2))
    for way, sign in enumerate((1, -1)):
        sums.emit(sign, whole, sums.own(sign, whole), *to(2, way, 1))
    yield CLOCK["end"]
    value = sums.own(0, whole)
    for k in (2, 3):
        for way in range(2):
            value = value + arrival(k, way)
    result[...] = value.astype(BF16)


def exchange(send, nz, nx, src, dst, send_sem, recv_sem):
    count = nz * nx
    me = lax.axis_index("z") * nx + lax.axis_index("x")

    def out(d):
        to = lax.rem(me + d, count)
        return send.copy(
            src.at[to], dst.at[me], send_sem.at[d], recv_sem.at[d], {"z": to // nx, "x": lax.rem(to, nx)}
        )

    @pl.loop(1, count)
    def _(d):
        out(d).start()

    def wait():
        @pl.loop(1, count)
        def _(d):
            origin = lax.rem(me + count - d, count)
            send.copy(
                src.at[origin], dst.at[origin], send_sem.at[d], recv_sem.at[d],
                {"z": origin // nx, "x": lax.rem(origin, nx)},
            ).wait_recv()

    def sent():
        @pl.loop(1, count)
        def _(d):
            out(d).wait_send()

    send.owed.append(sent)
    dst[me] = src[me]
    return wait


def kernel(sizes, *refs):
    nz, nx, ny, cap, spaced = sizes
    given, (mixer_out, expert_out) = refs[:COUNT_IN], refs[COUNT_IN : COUNT_IN + 2]
    inputs, scratch = refs[COUNT_IN + 2 : 2 * COUNT_IN + 2], refs[2 * COUNT_IN + 2 :]
    (routing, routing_weight, tokens, token_gain, query_latent, shared_latent, rotary_key, inside_cos, inside_sin,
     block_cos, block_sin, query_gain, shared_gain, plain_weight, turn_weight, key_weight, value_weight,
     gate, up, down, mixer_weight) = inputs
    (out_rows, in_rows, out_far, in_far, pack, mix_high, mix_low, gath, gate_up, hidden, part_e, given_e, ring_e,
     back_out, back_in, result_e, queries, query_1, query_2, keys, peak, total, accum, share_out, stat_out, share_in,
     stat_in, heads, part_m, given_m, ring_m,
     s_in, s_a, r_a, s_x, r_x, sp_x, rp_x, s_g, r_g, sp_g, rp_g, sp_e, rp_e, s_e, r_e, s_b, r_b, s_f, r_f, sp_f, rp_f,
     s_q, r_q, s_k, r_k, s_o, r_o, s_t, r_t, sp_m, rp_m, s_m, r_m, s_h, r_h, sp_h, rp_h) = scratch
    z, x, y, core = (lax.axis_index(a) for a in ("z", "x", "y", "c"))
    count = nz * nx
    me = z * nx + x
    turn = 2 * y + core
    rows = query_latent.shape[0]
    other = {"c": 1 - core}
    send = Sender()

    barrier = pltpu.get_barrier_semaphore()

    @pl.loop(1, count)
    def _(d):
        to = lax.rem(me + d, count)
        pl.semaphore_signal(
            barrier, inc=1, device_id={"z": to // nx, "x": lax.rem(to, nx)}, device_id_type=MESH
        )

    greeted = [{"y": lax.rem(y + d + ny, ny)} for d in ((1, -1, 2, -2) if ny == 8 else (1, -1))] + [other]
    for device in greeted:
        pl.semaphore_signal(barrier, inc=1, device_id=device, device_id_type=MESH)

    loads = [pltpu.make_async_copy(a, b, s_in.at[i]) for i, (a, b) in enumerate(zip(given, inputs))]
    for load in loads:
        load.start()

    def loaded(first, last):
        for load in loads[first:last]:
            load.wait()

    def gather_columns(ref, sems, start):
        def piece(p, lo, size):
            return ref.at[pl.ds(lo, size), pl.ds(pl.multiple_of((2 * p + core) * LANES, LANES), LANES)]

        def piece_other(p, lo, size):
            return ref.at[pl.ds(lo, size), pl.ds(pl.multiple_of((2 * p + 1 - core) * LANES, LANES), LANES)]

        if ny == 8:
            yield from near_gather(send, piece, piece_other, ref.shape[0], sems, other, start)
        else:
            pair = (other, *sems[2:])
            for _, when in ring_gather(send, "y", ny, piece, ref.shape[0], 2, *sems[:2], (start, 4.0, 4.0), pair):
                yield when
            for step in range(ny // 2 + 1):
                pair_arrived(send, ny, "y", piece_other, ref.shape[0], 2, step, pair)

    def expert_chain():
        width = pl.ds(pl.multiple_of(turn * LANES, LANES), LANES)
        far = lax.rem(y + ny // 2, ny)
        far_width = pl.ds(pl.multiple_of((2 * far + core) * LANES, LANES), LANES)
        loaded(0, 4)
        wide = tokens[...].astype(F32)
        factor = lax.rsqrt(jnp.mean(wide * wide, axis=-1, keepdims=True) + EPSILON)
        own, own_far = (
            (tokens[:, w].astype(F32) * factor * token_gain[:, w]).astype(BF16) for w in (width, far_width)
        )
        count_of = own.shape[0]
        named = iota((count, count_of), 0)
        member = jnp.zeros((count, count_of), F32)
        weight = jnp.zeros((count, count_of), F32)
        for k in range(routing.shape[0]):
            hit = routing[k : k + 1, :] == named
            member = member + jnp.where(hit, 1.0, 0.0)
            weight = weight + jnp.where(hit, routing_weight[k : k + 1, :], 0.0)
        member = member.astype(BF16)
        earlier = jnp.where(
            iota((count_of, count_of), 0) < iota((count_of, count_of), 1), 1.0, 0.0
        ).astype(BF16)
        rank = dot(member, earlier).astype(BF16)
        slots = count * spaced

        def block(line):
            return ((line.astype(F32) + 0.5) * (1.0 / spaced)).astype(jnp.int32)

        spread = jnp.where(block(iota((slots, count), 0)) == iota((slots, count), 1), 1.0, 0.0).astype(BF16)
        line = iota((slots, count_of), 0)
        place = (line - block(line) * spaced).astype(F32)
        chosen = (dot(spread, member) > 0.5) & (dot(spread, rank) == place)
        member_row = jnp.where(chosen, 1.0, 0.0).astype(BF16)
        out_rows[...] = dot(member_row, own).astype(BF16).reshape(out_rows.shape)
        yield 0.0
        arrive = exchange(send, nz, nx, out_rows, in_rows, s_a, r_a)
        yield CLOCK["more"]
        out_far[...] = dot(member_row, own_far).astype(BF16).reshape(out_far.shape)
        high = weight.astype(BF16)
        low = (weight - high.astype(F32)).astype(BF16)
        mix_high[...] = jnp.where(chosen, dot(spread, high), 0.0).astype(BF16)
        mix_low[...] = jnp.where(chosen, dot(spread, low), 0.0).astype(BF16)
        column = iota(pack.shape, 1)
        inner = column - block(column) * spaced
        goal = jnp.where(inner < cap, block(column) * cap + inner, -1)
        pack[...] = jnp.where(goal == iota(pack.shape, 0), 1.0, 0.0).astype(BF16)
        gate_up[...] = jnp.zeros_like(gate_up)
        yield CLOCK["arrive"]
        arrive()
        gath[turn] = dot(pack[...], in_rows[...].reshape(slots, LANES)).astype(BF16)
        slot = lambda p: 2 * p + core
        slot_other = lambda p: 2 * p + 1 - core
        packed = gath.shape[1]
        piece = lambda p, lo, size: gath.at[slot(p), pl.ds(lo, size)]
        piece_other = lambda p, lo, size: gath.at[slot_other(p), pl.ds(lo, size)]
        pair = (other, sp_g, rp_g)
        ring = ring_gather(send, "y", ny, piece, packed, PARTS, s_g, r_g, CLOCK["gather"], pair, False)
        ahead = next(ring, None)
        arrive_far = exchange(send, nz, nx, out_far, in_far, s_x, r_x)

        def consume(*pieces):
            lines = [pl.ds(pl.multiple_of(piece * LANES, LANES), LANES) for piece in pieces]
            both = jnp.concatenate(
                [jnp.concatenate([gate[at, :], up[at, :]], axis=1) for at in lines], axis=0
            )
            gate_up[...] += dot(jnp.concatenate([gath[piece] for piece in pieces], axis=1), both)

        def consume_step(step, which):
            consume(*(which(lax.rem(y + offset, ny)) for offset in sorted({-step % ny, step % ny})))

        far_slot, far_other = slot(far), slot_other(far)
        far_copy = (gath.at[far_slot], gath.at[far_slot], sp_x, rp_x, other)
        loaded(17, 19)
        consume_step(0, slot)
        for step in range(1, ny // 2 + 1):
            behind = step - 1
            while ahead is not None and ahead[0] == step:
                yield ahead[1]
                ahead = next(ring, None)
                if behind is not None:
                    pair_arrived(send, ny, "y", piece_other, packed, PARTS, behind, pair)
                    consume_step(behind, slot_other)
                    behind = None
            if behind is not None:
                pair_arrived(send, ny, "y", piece_other, packed, PARTS, behind, pair)
                consume_step(behind, slot_other)
            if step == max(1, ny // 2 - 2):
                arrive_far()
                gath[far_slot] = dot(pack[...], in_far[...].reshape(slots, LANES)).astype(BF16)
                send.start(*far_copy)
                consume(far_slot)
            if step < ny // 2:
                consume_step(step, slot)
        ref = gath.at[far_other]
        send.copy(ref, ref, sp_x, rp_x, other).wait_recv()
        consume(far_other)
        gate_pre = jnp.minimum(gate_up[:, :LANES], CLAMP_LIMIT)
        up_pre = jnp.clip(gate_up[:, LANES:], -CLAMP_LIMIT, CLAMP_LIMIT)
        hidden[...] = ((up_pre + 1.0) * (gate_pre * jax.nn.sigmoid(SLOPE * gate_pre))).astype(BF16)

        def product(p):
            return dot(hidden[...], down[:, pl.ds(pl.multiple_of(2 * LANES * p, 2 * LANES), 2 * LANES)])

        loaded(19, 20)
        early = len(send.owed)
        sums = PairSum(send, ny, product, part_e, given_e, (sp_e, rp_e), other)
        yield from ring_scatter(send, ny, sums, ring_e, PARTS, (s_e, r_e), result_e, CLOCK["scatter"])
        back_out[...] = dot(pack[...], result_e[...], 0, 0).astype(BF16).reshape(back_out.shape)
        arrive = exchange(send, nz, nx, back_out, back_in, s_b, r_b)
        send.finish(early)
        yield CLOCK["back"]
        arrive()
        back = back_in[...].reshape(slots, LANES)
        mixed = dot(mix_high[...], back, 0, 0) + dot(mix_low[...], back, 0, 0)
        expert_out[:, width] = mixed.astype(BF16)
        yield from gather_columns(expert_out, (s_f, r_f, sp_f, rp_f), CLOCK["last"])

    def mixer_chain():
        yield CLOCK["local"]
        scale = (NOPE + ROPE) ** -0.5 * math.log2(math.e)
        loaded(4, 17)
        mine = iota(block_cos.shape, 1) == me
        cos_b = jnp.sum(jnp.where(mine, block_cos[...], 0.0), axis=1, keepdims=True)
        sin_b = jnp.sum(jnp.where(mine, block_sin[...], 0.0), axis=1, keepdims=True)
        cosine = inside_cos[...] * cos_b - inside_sin[...] * sin_b
        sine = inside_sin[...] * cos_b + inside_cos[...] * sin_b
        latent = normed(query_latent, query_gain)
        queries[x, :rows] = dot(latent, plain_weight[...]).astype(BF16)
        raw = turned(dot(turn_weight[...], latent, 1, 1), cosine, sine)
        raw = jnp.concatenate([raw, jnp.zeros_like(raw)], axis=0)
        queries[x, rows:] = raw.T.astype(BF16)
        shared = normed(shared_latent, shared_gain)
        keys[z, :rows] = dot(shared, key_weight[...]).astype(BF16)
        keys[z, rows : 2 * rows] = dot(shared, value_weight[...]).astype(BF16)
        raw = turned(rotary_key[...].astype(F32), cosine, sine)
        raw = jnp.concatenate([raw[:, : rows // 2], raw[:, rows // 2 :]], axis=0)
        keys[z, 2 * rows :] = raw.T.astype(BF16)
        yield CLOCK["start"]
        keys_here.append(ring_gather(
            send, "z", nz, lambda p, lo, size: keys.at[p, pl.ds(lo, size)], keys.shape[1], 2, s_k, r_k, CLOCK["keys"]
        ))
        ahead.append(next(keys_here[0], None))
        to_x = [lax.rem(x + d, nx) for d in range(nx)]
        from_x = [lax.rem(x + nx - d, nx) for d in range(nx)]
        for d in range(1, nx):
            send.start(queries.at[x], queries.at[x], s_q.at[d], r_q.at[d], {"x": to_x[d]})
        yield CLOCK["queries"]
        for d in range(1, nx):
            ref = queries.at[from_x[d]]
            send.copy(ref, ref, s_q.at[d], r_q.at[d], {"x": to_x[d]}).wait_recv()
        move = jnp.where(iota((LANES, LANES), 0) + ROPE == iota((LANES, LANES), 1), 1.0, 0.0).astype(BF16)
        for j in range(nx):
            span = pl.ds(j * rows, rows)
            plain, turned_part = queries[j, :rows], queries[j, rows:]
            query_1[span, :LANES] = plain
            query_1[span, LANES:] = turned_part
            query_2[span, :LANES] = plain
            query_2[span, LANES:] = dot(turned_part, move).astype(BF16)

        def attend(piece, own):
            half = rows // 2
            both = keys[piece, 2 * rows :]
            key_1 = jnp.concatenate([keys[piece, :half], both], axis=1)
            key_2 = jnp.concatenate([keys[piece, half:rows], both], axis=1)
            scores = jnp.concatenate(
                [dot(key_1, query_1[...], 1, 1), dot(key_2, query_2[...], 1, 1)], axis=0
            )
            if own:
                visible = iota(scores.shape, 0) + rows * x <= iota(scores.shape, 1)
                scores = jnp.where(visible, scores, NEGATIVE)
            highest = jnp.max(scores, axis=0, keepdims=True)
            if not own:
                highest = jnp.maximum(highest, peak[...])
            probs = jnp.exp2((scores - highest) * scale)
            summed = jnp.sum(probs, axis=0, keepdims=True)
            mixed = dot(keys[piece, rows : 2 * rows], probs.astype(BF16), 0, 0)
            if own:
                total[...] = summed
                accum[...] = mixed
            else:
                fade = jnp.exp2((peak[...] - highest) * scale)
                total[...] = total[...] * fade + summed
                accum[...] = accum[...] * fade + mixed
            peak[...] = highest

        attend(z, True)
        steps = nz // 2
        for step in range(1, steps + 1):
            yield CLOCK["attend"][step - 1]
            while ahead[0] is not None and ahead[0][0] == step:
                ahead[0] = next(keys_here[0], None)

            @pl.when(z >= step)
            def _():
                attend(lax.rem(z - step + nz, nz), False)

            if step < steps:
                @pl.when(z + step >= nz)
                def _():
                    attend(lax.rem(z + step, nz), False)

        share = (accum[...] / total[...]).astype(BF16)
        for j in range(nx):
            span = slice(j * rows, (j + 1) * rows)
            share_out[j] = share[:, span]
            stat = (8, rows)
            stat_out[j] = jnp.where(iota(stat, 0) == 0, peak[:, span], total[:, span])
        for d in range(1, nx):
            device = {"x": to_x[d]}
            send.start(share_out.at[to_x[d]], share_in.at[x], s_o.at[d], r_o.at[d], device)
            send.start(stat_out.at[to_x[d]], stat_in.at[x], s_t.at[d], r_t.at[d], device)
        share_in[x] = share_out[x]
        stat_in[x] = stat_out[x]
        yield CLOCK["merge"]
        for d in range(1, nx):
            device = {"x": to_x[d]}
            for ref, s, r in ((share_in, s_o, r_o), (stat_in, s_t, r_t)):
                ref = ref.at[from_x[d]]
                send.copy(ref, ref, s.at[d], r.at[d], device).wait_recv()
        peaks = [stat_in[j, 0:1, :] for j in range(nx)]
        highest = functools.reduce(jnp.maximum, peaks)
        factors = [stat_in[j, 1:2, :] * jnp.exp2((peaks[j] - highest) * scale) for j in range(nx)]
        merged = sum(share_in[j].astype(F32) * factors[j] for j in range(nx)) / sum(factors)
        heads[...] = merged.astype(BF16)

        def product(p):
            columns = pl.ds(pl.multiple_of(2 * LANES * p, 2 * LANES), 2 * LANES)
            return dot(heads[...], mixer_weight[:, columns], 0, 0)

        loaded(20, 21)
        yield CLOCK["mixer"]
        sums = PairSum(send, ny, product, part_m, given_m, (sp_m, rp_m), other)
        result = mixer_out.at[:, pl.ds(pl.multiple_of(turn * LANES, LANES), LANES)]
        if ny == 8:
            yield from near_scatter(send, sums, ring_m, (s_m, r_m), result, CLOCK["mixer"])
        else:
            yield from ring_scatter(send, ny, sums, ring_m, 2, (s_m, r_m), result, (CLOCK["mixer"], 3.5, 3.5))
        yield from gather_columns(mixer_out, (s_h, r_h, sp_h, rp_h), CLOCK["mixer_gather"])

    keys_here, ahead = [], []

    def keys_chain():
        yield CLOCK["keys"][1][0]
        while ahead[0] is not None:
            ahead[0] = next(keys_here[0], None)
            if ahead[0] is not None:
                yield ahead[0][1]

    chains = [expert_chain(), keys_chain(), mixer_chain()]
    waiting = [(next(chain), i) for i, chain in enumerate(chains)]
    pl.semaphore_wait(barrier, count - 1 + len(greeted))
    while waiting:
        _, i = waiting.pop(waiting.index(min(waiting)))
        when = next(chains[i], None)
        if when is not None:
            waiting.append((when, i))
    send.finish()


def per_device(sizes, query_latent, shared_latent, rotary_key, query_gain, shared_gain, plain_weight, turn_weight,
               key_weight, value_weight, mixer_weight, tokens, token_gain, routing, routing_weight, gate, up, down):
    nz, nx, ny, cap, spaced = sizes
    rows = query_latent.shape[0]
    count, pieces = nz * nx, 2 * ny
    frequency = ROTARY_BASE ** (-2.0 * np.arange(ROPE // 2) / ROPE)
    inside = frequency[:, None] * np.arange(rows)
    blocks = frequency[:, None] * (np.arange(count) * rows)
    tables = [jnp.asarray(f(a), F32) for a in (inside, blocks) for f in (np.cos, np.sin)]
    slots, packed = count * spaced, count * cap
    count_of = tokens.shape[0]
    vmem, dma = pltpu.VMEM, pltpu.SemaphoreType.DMA
    hops, handed = dma((2, ny // 2, PARTS)), dma((2, ny // 2 + 1, PARTS))
    if ny == 8:
        hops_m, hops_h, handed_h = dma((2, 4)), dma((2, 4)), dma((2, 5))
    else:
        hops_m, hops_h, handed_h = hops, hops, handed
    scratch = [
        vmem((count, spaced, LANES), BF16), vmem((count, spaced, LANES), BF16),
        vmem((count, spaced, LANES), BF16), vmem((count, spaced, LANES), BF16), vmem((packed, slots), BF16),
        vmem((slots, count_of), BF16), vmem((slots, count_of), BF16), vmem((pieces, packed, LANES), BF16),
        vmem((packed, 2 * LANES), F32), vmem((packed, LANES), BF16), vmem((2, ny, packed, LANES), BF16),
        vmem((ny, packed, LANES), BF16), vmem((2, ny // 2, packed, LANES), BF16),
        vmem((count, spaced, LANES), BF16), vmem((count, spaced, LANES), BF16), vmem((packed, LANES), BF16),
        vmem((nx, 2 * rows, LANES), BF16), vmem((nx * rows, 2 * LANES), BF16), vmem((nx * rows, 2 * LANES), BF16),
        vmem((nz, 2 * rows + rows // 2, LANES), BF16), vmem((1, nx * rows), F32), vmem((1, nx * rows), F32),
        vmem((LANES, nx * rows), F32), vmem((nx, LANES, rows), BF16), vmem((nx, 8, rows), F32),
        vmem((nx, LANES, rows), BF16), vmem((nx, 8, rows), F32), vmem((LANES, rows), BF16),
        vmem((2, ny, rows, LANES), BF16), vmem((ny, rows, LANES), BF16), vmem((2, ny // 2, rows, LANES), BF16),
        dma((COUNT_IN,)), dma((count,)), dma((count,)), dma((count,)), dma((count,)), dma, dma,
        hops, hops, handed, handed, dma((ny,)), dma((ny,)), hops, hops,
        dma((count,)), dma((count,)), hops_h, hops_h, handed_h, handed_h,
        dma((nx,)), dma((nx,)), dma((2, nz // 2, 2)), dma((2, nz // 2, 2)), dma((nx,)), dma((nx,)), dma((nx,)),
        dma((nx,)), dma((ny,)), dma((ny,)), hops_m, hops_m, hops_h, hops_h, handed_h, handed_h,
    ]
    spec = pl.BlockSpec(memory_space=pltpu.VMEM)
    operands = (
        routing.T, routing_weight.T, tokens, token_gain[None], query_latent, shared_latent, rotary_key.T, *tables,
        query_gain, shared_gain[None], plain_weight, turn_weight.T, key_weight, value_weight,
        gate[0], up[0], down[0], mixer_weight,
    )
    scratch = [vmem(a.shape, a.dtype) for a in operands] + scratch
    return pl.pallas_call(
        functools.partial(kernel, sizes),
        out_shape=(
            pltpu.VMEM((rows, pieces * LANES), BF16),
            pltpu.VMEM((count_of, pieces * LANES), BF16),
        ),
        in_specs=[pl.BlockSpec(memory_space=pltpu.HBM)] * len(operands),
        out_specs=(spec, spec),
        scratch_shapes=scratch,
        compiler_params=pltpu.CompilerParams(
            collective_id=0, has_side_effects=True, vmem_limit_bytes=56 * 1024 * 1024
        ),
        name="step",
    )(*operands)


def build(mesh, nx, cap, spaced):
    nz, ny = mesh.shape["ep"] // nx, mesh.shape["tp"] // 2
    finer = Mesh(mesh.devices.reshape(nz, nx, ny, 2), ("z", "x", "y", "c"))
    placed = (
        P(EP, None), P(EP, None), P(EP, None), P(), P(), P(None, TP), P(None, TP), P(None, TP), P(None, TP),
        P(TP, None), P(EP, None), P(), P(EP, None), P(EP, None), P(EP, None, TP), P(EP, None, TP), P(EP, TP, None),
    )
    return jax.shard_map(
        functools.partial(per_device, (nz, nx, ny, cap, spaced)),
        mesh=finer, in_specs=placed, out_specs=(P(EP, None), P(EP, None)), check_vma=False,
    )


def solution(mesh):
    return build(mesh, NX, 21, 24)
```
